32 devices in a mesh: sp: 8 (over z, y), tp: 4 (over x, core).
Axes of the slice: x: 2, y: 2, z: 4, core: 2. Of those that a mesh axis runs over, the one named last changes fastest.
Arguments:
- target: bfloat16 [1024, 2048], P('sp'), may hold values from -160 to 160
- source: bfloat16 [2048, 2048], P(('sp', 'tp')), may hold values from -160 to 160
- query_gain: float32 [2048], replicated, may hold values from 0.1 to 1.9
- source_gain: float32 [2048], replicated, may hold values from 0.1 to 1.9
- query_weight: bfloat16 [2048, 2048], P(None, 'tp'), may hold values from -4 to 4
- key_weight: bfloat16 [2048, 512], replicated, may hold values from -4 to 4
- value_weight: bfloat16 [2048, 512], replicated, may hold values from -1 to 1
- out_weight: bfloat16 [2048, 2048], P('tp'), may hold values from -0.125 to 0.125
- mixer_gain: float32 [2048], replicated, may hold values from 0.1 to 1.9
- gate_weight: bfloat16 [2048, 3072], P(None, 'tp'), may hold values from -0.125 to 0.125
- up_weight: bfloat16 [2048, 3072], P(None, 'tp'), may hold values from -0.125 to 0.125
- gate_taps: bfloat16 [3, 3072], P(None, 'tp'), may hold values from -3.5 to 3.5
- up_taps: bfloat16 [3, 3072], P(None, 'tp'), may hold values from -3.5 to 3.5
- down_weight: bfloat16 [3072, 2048], P('tp'), may hold values from -0.109375 to 0.109375
- final_gain: float32 [2048], replicated, may hold values from 0.1 to 1.9
Outputs:
- layer_out: bfloat16 [1024, 2048], P(('sp', 'tp'))
The draws below stay inside these ranges and needn't reach their ends.
All inputs are finite; a program needn't handle non-finite values.
Results may differ from the reference program's by a relative error of at most 0.012.
Values may be sent and summed in bfloat16 or wider, within the bound.
A program may use at most 64 MiB of HBM per device.

```python
import math
import jax
import jax.numpy as jnp
from jax import lax

D = 2048
HEADS = 8
HEAD = 256
KV_HEADS = 2
FF = 3072
CONV = 3
TGT_DEV = 128
SRC_DEV = 256
TGT = 1024
SRC = 2048
N_SP = 8
N_TP = 4


def draw_target(key, part):
    result = jax.random.truncated_normal(jax.random.fold_in(key, 11), -4.0, 4.0, (TGT, D), jnp.float32)
    return result.astype(jnp.bfloat16)


def draw_source(key, part):
    result = jax.random.truncated_normal(jax.random.fold_in(key, 31), -4.0, 4.0, (SRC, D), jnp.float32)
    return result.astype(jnp.bfloat16)


def drawn_weight(key, salt, columns):
    drawn = jax.random.truncated_normal(jax.random.fold_in(key, salt), -4.0, 4.0, (D, columns), jnp.float32)
    drawn = drawn * math.sqrt(2.5 / D)
    return drawn.astype(jnp.bfloat16)


def draw_query_weight(key, part):
    return drawn_weight(key, 21, HEADS * HEAD)


def draw_key_weight(key, part):
    return drawn_weight(key, 22, KV_HEADS * HEAD)


def block_scale(own_key, dims, shards, low, top_value):
    level, own = 1.0, jax.random.fold_in(own_key, 6)
    for axis_at, blocks in shards:
        heights = jnp.exp(jax.random.uniform(jax.random.fold_in(own, axis_at), (blocks,), jnp.float32, low / len(shards), top_value / len(shards)))
        level = level * jnp.repeat(heights, dims[axis_at] // blocks).reshape([-1 if axis == axis_at else 1 for axis in range(len(dims))])
    return level


def noise(key, dims, spread, reach, split=(), dtype=jnp.bfloat16):
    entries = spread * jax.random.normal(key, dims, jnp.float32)
    if split:
        entries = entries * block_scale(key, dims, split, -0.22, 0.18)
    return jnp.clip(entries, -reach, reach).astype(dtype)


def setup_inputs(seed: int = 0) -> dict:
    key_of = jax.random.split(jax.random.key(seed), 16)
    target = draw_target(jax.random.fold_in(key_of[15], 71), 0)
    source = draw_source(jax.random.fold_in(key_of[15], 71), 0)
    query_gain = jnp.clip(1.0 + 0.18 * jax.random.normal(key_of[2], (D,), jnp.float32), 0.1, 1.9)
    source_gain = jnp.clip(1.0 + 0.18 * jax.random.normal(key_of[3], (D,), jnp.float32), 0.1, 1.9)
    query_weight = draw_query_weight(jax.random.fold_in(key_of[15], 71), 0)
    key_weight = draw_key_weight(jax.random.fold_in(key_of[15], 71), 0)
    value_weight = noise(key_of[6], (D, KV_HEADS * HEAD), (D // 48) ** -0.5, 1.0)
    out_weight = noise(key_of[7], (HEADS * HEAD, D), (HEADS * HEAD) ** -0.5, 0.125, ((0, 4),))
    mixer_gain = jnp.clip(1.0 + 0.18 * jax.random.normal(key_of[8], (D,), jnp.float32), 0.1, 1.9)
    gate_weight = noise(key_of[9], (D, FF), D ** -0.5, 0.125, ((1, 4),))
    up_weight = noise(key_of[10], (D, FF), D ** -0.5, 0.125, ((1, 4),))
    gate_taps = noise(key_of[11], (CONV, FF), CONV ** -0.5, 3.5, ((1, 4),))
    up_taps = noise(key_of[12], (CONV, FF), CONV ** -0.5, 3.5, ((1, 4),))
    down_weight = noise(key_of[13], (FF, D), FF ** -0.5, 0.109375, ((0, 4),))
    final_gain = jnp.clip(1.0 + 0.18 * jax.random.normal(key_of[14], (D,), jnp.float32), 0.1, 1.9)
    return {"target": target, "source": source, "query_gain": query_gain, "source_gain": source_gain, "query_weight": query_weight, "key_weight": key_weight, "value_weight": value_weight, "out_weight": out_weight, "mixer_gain": mixer_gain, "gate_weight": gate_weight, "up_weight": up_weight, "gate_taps": gate_taps, "up_taps": up_taps, "down_weight": down_weight, "final_gain": final_gain}


EPS = 1e-06

def normalize(values, gain):
    widened = values.astype(jnp.float32)
    scaled = widened * lax.rsqrt(lax.optimization_barrier(jnp.mean(widened * widened, axis=-1, keepdims=True)) + EPS)
    return (scaled * gain.astype(jnp.float32)).astype(jnp.bfloat16)

def rounded(values):
    return lax.optimization_barrier(values.astype(jnp.bfloat16)).astype(jnp.float32)

def reference(target, source, query_gain, source_gain, query_weight, key_weight, value_weight, out_weight, mixer_gain, gate_weight, up_weight, gate_taps, up_taps, down_weight, final_gain):
    group_size = HEADS // KV_HEADS
    slice_rows = SRC_DEV // N_TP
    normed = normalize(target, query_gain)
    queries = rounded(jnp.dot(normed, query_weight, preferred_element_type=jnp.float32))
    source_normed = normalize(source, source_gain)
    key_rows = rounded(jnp.dot(source_normed, key_weight, preferred_element_type=jnp.float32))
    value_rows = rounded(jnp.dot(source_normed, value_weight, preferred_element_type=jnp.float32))
    key_slices = key_rows.reshape(N_SP, N_TP, slice_rows, KV_HEADS, HEAD)
    value_slices = value_rows.reshape(N_SP, N_TP, slice_rows, KV_HEADS, HEAD)
    query_blocks = queries.reshape(N_SP, TGT_DEV, KV_HEADS, group_size, HEAD)
    score_scale = HEAD ** (-0.5)

    def attend(query_block):
        maxima = []
        sums = []
        partial_sums = []
        for slot in range(N_TP):
            slot_keys = key_slices[:, slot].reshape(N_SP * slice_rows, KV_HEADS, HEAD)
            slot_values = value_slices[:, slot].reshape(N_SP * slice_rows, KV_HEADS, HEAD)
            scores = jnp.einsum('bgjd,ngd->gjbn', query_block, slot_keys) * score_scale
            highest = lax.optimization_barrier(jnp.max(scores, axis=-1))
            weights = jnp.exp(scores - highest[..., None])
            maxima.append(highest)
            sums.append(lax.optimization_barrier(jnp.sum(weights, axis=-1)))
            partial_sums.append(jnp.einsum('gjbn,ngd->gjbd', rounded(weights), slot_values))
        maxima = jnp.stack(maxima)
        sums = jnp.stack(sums)
        partial_sums = jnp.stack(partial_sums)
        overall = lax.optimization_barrier(jnp.max(maxima, axis=0))
        factor = jnp.exp(maxima - overall)
        denominator = lax.optimization_barrier(jnp.sum(factor * sums, axis=0))
        merged = lax.optimization_barrier(jnp.sum(factor[..., None] * partial_sums, axis=0)) / denominator[..., None]
        return merged.transpose(2, 0, 1, 3).reshape(TGT_DEV, HEADS * HEAD).astype(jnp.bfloat16)
    attended = lax.map(attend, query_blocks).reshape(N_SP * TGT_DEV, HEADS * HEAD)
    projected = jnp.dot(attended, out_weight, preferred_element_type=jnp.float32)
    residual = (target.astype(jnp.float32) + projected).astype(jnp.bfloat16)
    mixer_in = normalize(residual, mixer_gain)
    gate_rows = rounded(jnp.dot(mixer_in, gate_weight, preferred_element_type=jnp.float32))
    up_rows = rounded(jnp.dot(mixer_in, up_weight, preferred_element_type=jnp.float32))
    stacked = jnp.stack([gate_rows, up_rows])
    padded = jnp.pad(stacked, ((0, 0), (CONV - 1, 0), (0, 0)))
    conv_taps = jnp.stack([gate_taps, up_taps]).astype(jnp.float32)
    total_rows = N_SP * TGT_DEV
    mixed = conv_taps[:, 0:1, :] * padded[:, 0:total_rows, :]
    for index_tap in range(1, CONV):
        mixed = mixed + conv_taps[:, index_tap:index_tap + 1, :] * padded[:, index_tap:index_tap + total_rows, :]
    hidden = (jax.nn.silu(mixed[0]) * mixed[1]).astype(jnp.bfloat16)
    mixer = jnp.dot(hidden, down_weight, preferred_element_type=jnp.float32)
    return normalize(residual.astype(jnp.float32) + mixer, final_gain)
```

```python
import functools

import jax
import jax.numpy as jnp
from jax import lax
from jax.experimental import pallas as pl
from jax.experimental.pallas import tpu as pltpu
from jax.sharding import PartitionSpec as P

MESH = pl.DeviceIdType.MESH
EPS = 1e-06
HALO = 16
RUN = 32
CORES = 2
F32 = jnp.float32
BF16 = jnp.bfloat16


def normed(values, gain):
    wide = values.astype(F32)
    scale = lax.rsqrt(jnp.mean(wide * wide, axis=-1, keepdims=True) + EPS)
    return (wide * scale * gain).astype(BF16)


def layer(
    dims,
    target_h,
    source_h,
    qgain_h,
    sgain_h,
    qw_h,
    kw_h,
    vw_h,
    ow_h,
    mgain_h,
    gw_h,
    uw_h,
    gtaps_h,
    utaps_h,
    dw_h,
    fgain_h,
    out_ref,
    tgt,
    src,
    qgain,
    sgain,
    qw,
    kw,
    vw,
    ow,
    mgain,
    gw,
    uw,
    gtaps,
    utaps,
    dw,
    fgain,
    kvh,
    kv,
    q2,
    top,
    tot,
    acc,
    att,
    part,
    half_s,
    half_r,
    chip_s,
    chip_r,
    own_t,
    res,
    rows_in,
    row_scale,
    halo_s,
    halo_r,
    conv_g,
    conv_u,
    hid,
    tail_s,
    tail_r,
    end_s,
    end_r,
    load_sem,
    kx_s,
    kx_r,
    ring_s,
    ring_r,
    d2_s,
    d2_r,
    b_s,
    b_r,
    bx_s,
    bx_r,
    m_s,
    m_r,
    rs_s,
    rs_r,
    h_s,
    h_r,
    f_s,
    f_r,
    fx_s,
    fx_r,
):
    n, chips, kv_heads, head, heads_here, cols, sub, wide = dims
    tgt_rows, width = tgt.shape
    r = src.shape[0]
    rs = tgt_rows // (CORES * chips)
    half_rows = chips * rs
    run = r // sub
    runs = chips * sub
    chunks = width // cols
    sp = lax.axis_index("sp")
    tp = lax.axis_index("tp")
    chip = tp // CORES
    core = tp % CORES
    mate = tp + 1 - 2 * core

    def chip_at(k):
        return (chip + k) % chips

    def ring_at(p):
        if n % 2:
            return p
        upper = p // (n // 2)
        return 2 * (p * (1 - upper) + (n - 1 - p) * upper) + upper

    if n % 2:
        pos = sp
    else:
        pos = (sp // 2) * (1 - sp % 2) + (n - 1 - sp // 2) * (sp % 2)
    ahead = ring_at((pos + 1) % n)
    behind = ring_at((pos + n - 1) % n)

    def load(index, hbm, vmem):
        copy = pltpu.make_async_copy(hbm, vmem, load_sem.at[index])
        copy.start()
        return copy

    def head_of(c):
        return (c * CORES * kv_heads) // (chips * CORES)

    own_head = head_of(chip)
    order = [(own_head + 1 + g) % kv_heads for g in range(kv_heads)]

    def columns(g):
        return pl.ds(pl.multiple_of(g * head, head), head)

    first = [load(0, source_h, src), load(1, sgain_h, sgain)]
    by_head = [
        [
            load(2 + 2 * i, kw_h.at[:, columns(g)], kw.at[:, columns(g)]),
            load(3 + 2 * i, vw_h.at[:, columns(g)], vw.at[:, columns(g)]),
        ]
        for i, g in enumerate(order)
    ]
    used = 2 + 2 * kv_heads

    barrier = pltpu.get_barrier_semaphore()
    following = (sp + 1) % n
    peers = [(ahead, tp), (behind, tp), (sp, mate)]
    peers += [(sp, chip_at(k) * CORES + core) for k in range(1, chips)]
    for peer in peers:
        pl.semaphore_signal(barrier, inc=1, device_id=peer, device_id_type=MESH)

    def remote(source_ref, dest_ref, send, recv, device):
        return pltpu.make_async_remote_copy(
            src_ref=source_ref,
            dst_ref=dest_ref,
            send_sem=send,
            recv_sem=recv,
            device_id=device,
            device_id_type=MESH,
        )

    def block(slot, lineage, j):
        start = ((slot * CORES + lineage) * runs + j) * run
        if not isinstance(start, int):
            start = pl.multiple_of(start, run)
        return kv.at[pl.ds(start, run), :]

    def chip_copy(j):
        there = chip_at(j // sub)
        return remote(
            kvh.at[head_of(there), (j % sub) * run : (j % sub + 1) * run, :],
            block(0, core, j),
            kx_s.at[j],
            kx_r.at[j],
            (sp, there * CORES + core),
        )

    last = n // 2 if n % 2 == 0 else 0
    full = (n - 1) // 2
    own = range(sub)
    far = range(sub, runs)
    onward = ahead * (1 - core) + behind * core

    def slot_of(d, side):
        if isinstance(d, int) and d == 0:
            return 0
        if isinstance(d, int) and d == last:
            return n - 1
        return 2 * d - 1 + side

    def ring_copy(d, rel, j):
        lineage = core * (1 - rel) + (1 - core) * rel
        return remote(
            block(slot_of(d - 1, core), lineage, j),
            block(slot_of(d, core), lineage, j),
            ring_s.at[d, rel, j],
            ring_r.at[d, rel, j],
            (onward, tp),
        )

    def mirror_copy(d, rel, j, side):
        lineage = side * (1 - rel) + (1 - side) * rel
        held = block(slot_of(d, side), lineage, j)
        return remote(held, held, d2_s.at[d, rel, j], d2_r.at[d, rel, j], (sp, mate))

    def mirror_out(d, rel, j):
        return mirror_copy(d, rel, j, core)

    def mirror_in(d, rel, j):
        return mirror_copy(d, rel, j, 1 - core)

    def launch(j):
        if n > 1:
            ring_copy(1, 0, j).start()
        mirror_out(0, 0, j).start()

    def launch_mate(blocks):
        for j in blocks:
            mirror_in(0, 0, j).wait_recv()
            if full >= 1:
                ring_copy(1, 1, j).start()

    def launch_far():
        for j in far:
            chip_copy(j).wait_recv()
            launch(j)

    def arrive(d, rel, blocks):
        end = isinstance(d, int) and d == full
        for j in blocks:
            ring_copy(d, rel, j).wait_recv()
            if not end or (last and rel == 0):
                ring_copy(d + 1, rel, j).start()
            mirror_out(d, rel, j).start()

    def arrive_last(blocks):
        if last:
            for j in blocks:
                ring_copy(last, 0, j).wait_recv()
                mirror_out(last, 0, j).start()

    for copy in first:
        copy.wait()
    source_in = normed(src[...], sgain[...])
    second = [
        load(used + i, a, b)
        for i, (a, b) in enumerate(((target_h, tgt), (qgain_h, qgain), (qw_h, qw)))
    ]
    early = chips == kv_heads
    for i, g in enumerate(order):
        for copy in by_head[i]:
            copy.wait()
        keys = jnp.dot(source_in, kw[:, columns(g)], preferred_element_type=F32)
        kvh[g, :, :head] = keys.astype(BF16)
        values = jnp.dot(source_in, vw[:, columns(g)], preferred_element_type=F32)
        kvh[g, :, head:] = values.astype(BF16)
        if i == (kv_heads - 2 if early else kv_heads - 1):
            pl.semaphore_wait(barrier, len(peers))
            for j in range(sub, runs):
                chip_copy(j).start()
    kv[pl.ds(pl.multiple_of(core * chips * r, r), r), :] = kvh[own_head]
    for j in range(sub):
        launch(j)
    for copy in second:
        copy.wait()
    queries = jnp.dot(normed(tgt[...], qgain[...]), qw[...], preferred_element_type=F32).astype(
        BF16
    )
    for h in range(heads_here):
        q2[h * tgt_rows : (h + 1) * tgt_rows, :] = queries[:, h * head : (h + 1) * head]
    for k in range(chips):
        at = pl.ds(pl.multiple_of((k * CORES + core) * rs, rs), rs)
        own_t[k * rs : (k + 1) * rs, :] = tgt[at, :]
    top[...] = jnp.full(top.shape, -1e30, F32)
    tot[...] = jnp.zeros(tot.shape, F32)
    acc[...] = jnp.zeros(acc.shape, F32)

    slot_rows = CORES * chips * r

    def attend(slot, slots):
        start = slot * slot_rows
        if not isinstance(start, int):
            start = pl.multiple_of(start, slot_rows)
        here = pl.ds(start, slots * slot_rows)
        scores = lax.dot_general(
            q2[...], kv[here, :head], (((1,), (1,)), ((), ())), preferred_element_type=F32
        ) * (head**-0.5)
        old = top[...]
        new = jnp.maximum(old, jnp.max(scores, axis=-1, keepdims=True))
        shrink = jnp.exp(old - new)
        probs = jnp.exp(scores - new)
        top[...] = new
        tot[...] = tot[...] * shrink + jnp.sum(probs, axis=-1, keepdims=True)
        acc[...] = acc[...] * shrink + jnp.dot(
            probs.astype(BF16), kv[here, head:], preferred_element_type=F32
        )

    def mirrored(d):
        for rel in range(1 if isinstance(d, int) and d == last else CORES):
            for j in range(runs):
                mirror_in(d, rel, j).wait_recv()

    def wave(d):
        for blocks in (own, far):
            for rel in range(CORES):
                arrive(d, rel, blocks)

    if full >= 1:
        launch_mate(own)
        launch_far()
        launch_mate(far)
        wave(1)
        rest = [
            load(used + 3 + i, a, b)
            for i, (a, b) in enumerate(
                (
                    (ow_h, ow),
                    (mgain_h, mgain),
                    (gw_h, gw),
                    (uw_h, uw),
                    (gtaps_h, gtaps),
                    (utaps_h, utaps),
                    (dw_h, dw),
                    (fgain_h, fgain),
                )
            )
        ]
        done = 1
        if full > 4:
            wave(2)
            attend(0, 1)

            def middle(d, carry):
                wave(d)
                mirrored(d - 2)
                attend(2 * d - 5, 2)
                return carry

            lax.fori_loop(3, full, middle, 0)
            wave(full)
            done = full - 2
        else:
            for d in range(2, full + 1):
                wave(d)
        start = 2 * done - 1 if full > 4 else 0
        for d in range(done, full):
            mirrored(d)
        attend(start, 2 * full - 1 - start)
        arrive_last(range(runs))
        mirrored(full)
        attend(2 * full - 1, 2)
    else:
        rest = [
            load(used + 3 + i, a, b)
            for i, (a, b) in enumerate(
                (
                    (ow_h, ow),
                    (mgain_h, mgain),
                    (gw_h, gw),
                    (uw_h, uw),
                    (gtaps_h, gtaps),
                    (utaps_h, utaps),
                    (dw_h, dw),
                    (fgain_h, fgain),
                )
            )
        ]
        launch_far()
        launch_mate(range(runs))
        arrive_last(range(runs))
        attend(0, 1)
    if last:
        mirrored(last)
        attend(n - 1, 1)

    attended = (acc[...] / tot[...]).astype(BF16)
    for h in range(heads_here):
        att[:, h * head : (h + 1) * head] = attended[h * tgt_rows : (h + 1) * tgt_rows, :]
    for copy in rest:
        copy.wait()

    def piece(c, side):
        return pl.ds(pl.multiple_of((c * CORES + side) * rs, rs), rs)

    def multiply_out(lhs, weight, send, recv, send_sem, recv_sem):
        for c in range(chunks):
            here = slice(c * cols, (c + 1) * cols)
            part[c] = jnp.dot(lhs, weight[:, here], preferred_element_type=F32)
            for k in range(chips):
                send[c, k * rs : (k + 1) * rs, :] = part[c, piece(k, 1 - core), :].astype(BF16)
            remote(send.at[c], recv.at[c], send_sem.at[c], recv_sem.at[c], (sp, mate)).start()

    def mate_wait(c, send, recv, send_sem, recv_sem):
        remote(send.at[c], recv.at[c], send_sem.at[c], recv_sem.at[c], (sp, mate)).wait_recv()

    multiply_out(att[...], ow, half_s, half_r, b_s, b_r)

    body_rows = half_rows - HALO
    body = slice(0, body_rows)
    tail = slice(body_rows, half_rows)

    def wide_copy(k, c, i):
        at = (body, tail)[i]
        return remote(
            chip_s.at[c, at, :],
            chip_r.at[k - 1, c, at, :],
            bx_s.at[k, c, i],
            bx_r.at[k, c, i],
            (sp, chip_at(k) * CORES + core),
        )

    for c in range(chunks):
        mate_wait(c, half_s, half_r, b_s, b_r)
        here = slice(c * cols, (c + 1) * cols)
        for k in range(chips):
            at = slice(k * rs, (k + 1) * rs)
            both = part[c, piece(k, core), :] + half_r[c, at, :].astype(F32)
            res[at, here] = both + own_t[at, here].astype(F32)
            chip_s[c, at, :] = both.astype(BF16)
        for k in range(1, chips):
            wide_copy(k, c, 1).start()
    for c in range(chunks):
        for k in range(1, chips):
            wide_copy(k, c, 0).start()

    def settle(c, i):
        at = (body, tail)[i]
        here = slice(c * cols, (c + 1) * cols)
        residual = res[at, here]
        for k in range(1, chips):
            wide_copy(k, c, i).wait_recv()
            residual = residual + chip_r[k - 1, c, at, :].astype(F32)
        residual = residual.astype(BF16).astype(F32)
        res[at, here] = residual
        return jnp.sum(residual * residual, axis=-1, keepdims=True)

    def spot(k, side):
        return pl.ds(pl.multiple_of((k * CORES + side) * rs, rs), rs)

    def row_copy(c, k, side):
        held = rows_in.at[c, spot(k, side), :]
        return remote(held, held, m_s.at[c, k], m_r.at[c, k], (sp, mate))

    def scale_copy(k, side):
        held = row_scale.at[spot(k, side), :]
        return remote(held, held, rs_s.at[k], rs_r.at[k], (sp, mate))

    def halo_copy(i, t):
        return remote(halo_s, halo_r, h_s.at[i], h_r, (following, t))

    sends_halo = jnp.logical_and(core == 1, sp < n - 1)
    tail_squares = settle(0, 1)
    for c in range(1, chunks):
        tail_squares = tail_squares + settle(c, 1)
    scale = lax.rsqrt(tail_squares / width + EPS)
    for c in range(chunks):
        here = slice(c * cols, (c + 1) * cols)
        halo_s[c] = (res[tail, here] * scale * mgain[:, here]).astype(BF16)

    @pl.when(sends_halo)
    def _():
        halo_copy(0, mate).start()
        halo_copy(1, tp).start()

    def mix(c):
        for k in range(chips):
            row_copy(c, k, 1 - core).wait_recv()
        here = slice(c * cols, (c + 1) * cols)
        for weight, total in ((gw, conv_g), (uw, conv_u)):
            product = jnp.dot(rows_in[c], weight[here, :], preferred_element_type=F32)
            if c > 0:
                product = product + total[HALO:, :]
            total[HALO:, :] = product

    squares = jnp.zeros((body_rows, 1), F32)
    for c in range(chunks):
        squares = squares + settle(c, 0)
        here = slice(c * cols, (c + 1) * cols)
        for k in range(chips):
            at = slice(k * rs, (k + 1) * rs)
            rows_in[c, spot(k, core), :] = (res[at, here] * mgain[:, here]).astype(BF16)
            row_copy(c, k, core).start()
        if c > 0:
            mix(c - 1)
    squares = jnp.concatenate([squares, tail_squares], axis=0)
    scale = jnp.broadcast_to(lax.rsqrt(squares / width + EPS), (half_rows, row_scale.shape[1]))
    for k in range(chips):
        row_scale[spot(k, core), :] = scale[k * rs : (k + 1) * rs, :]
        scale_copy(k, core).start()

    @pl.when(sp == 0)
    def _():
        halo_r[...] = jnp.zeros(halo_r.shape, BF16)

    @pl.when(sp > 0)
    def _():
        halo_copy(0, tp).wait_recv()

    for weight, total in ((gw, conv_g), (uw, conv_u)):
        product = jnp.zeros((HALO, weight.shape[1]), F32)
        for c in range(chunks):
            product = product + jnp.dot(
                halo_r[c], weight[c * cols : (c + 1) * cols, :], preferred_element_type=F32
            )
        total[:HALO, :] = product.astype(BF16).astype(F32)
    mix(chunks - 1)
    for k in range(chips):
        scale_copy(k, 1 - core).wait_recv()

    hidden_cols = hid.shape[1]
    taps = gtaps.shape[0]
    for f in range(hidden_cols // wide):
        here = slice(f * wide, (f + 1) * wide)
        scale = row_scale[:, :1]
        for total in (conv_g, conv_u):
            total[HALO:, here] = (total[HALO:, here] * scale).astype(BF16).astype(F32)
        gate = jnp.zeros((tgt_rows, wide), F32)
        up = jnp.zeros((tgt_rows, wide), F32)
        for t in range(taps):
            begin = HALO - (taps - 1) + t
            rows = slice(begin, begin + tgt_rows)
            gate = gate + gtaps[t : t + 1, here].astype(F32) * conv_g[rows, here]
            up = up + utaps[t : t + 1, here].astype(F32) * conv_u[rows, here]
        hid[:, here] = (gate / (1.0 + jnp.exp(-gate)) * up).astype(BF16)

    multiply_out(hid[...], dw, tail_s, tail_r, f_s, f_r)

    def end_copy(k, c):
        there = chip_at(k)
        at = pl.ds(pl.multiple_of(there * rs, rs), rs)
        return remote(
            end_s.at[c, at, :],
            end_r.at[k - 1, c],
            fx_s.at[k, c],
            fx_r.at[k, c],
            (sp, there * CORES + core),
        )

    for c in range(chunks):
        mate_wait(c, tail_s, tail_r, f_s, f_r)
        for k in range(chips):
            at = slice(k * rs, (k + 1) * rs)
            both = part[c, piece(k, core), :] + tail_r[c, at, :].astype(F32)
            part[c, piece(k, core), :] = both
            end_s[c, at, :] = both.astype(BF16)
        for k in range(1, chips):
            end_copy(k, c).start()
    own = pl.ds(pl.multiple_of(chip * rs, rs), rs)
    squares = jnp.zeros((rs, 1), F32)
    sums = []
    for c in range(chunks):
        here = slice(c * cols, (c + 1) * cols)
        total = res[own, here] + part[c, piece(chip, core), :]
        for k in range(1, chips):
            end_copy(k, c).wait_recv()
            total = total + end_r[k - 1, c].astype(F32)
        squares = squares + jnp.sum(total * total, axis=-1, keepdims=True)
        sums.append(total)
    scale = lax.rsqrt(squares / width + EPS)
    for c in range(chunks):
        here = slice(c * cols, (c + 1) * cols)
        out_ref[:, here] = (sums[c] * scale * fgain[:, here]).astype(BF16)

    for j in range(sub, runs):
        chip_copy(j).wait_send()
    for k in range(1, chips):
        for c in range(chunks):
            wide_copy(k, c, 0).wait_send()
            wide_copy(k, c, 1).wait_send()
            end_copy(k, c).wait_send()
    for c in range(chunks):
        remote(half_s.at[c], half_r.at[c], b_s.at[c], b_r.at[c], (sp, mate)).wait_send()
        remote(tail_s.at[c], tail_r.at[c], f_s.at[c], f_r.at[c], (sp, mate)).wait_send()
    for k in range(chips):
        scale_copy(k, core).wait_send()
        for c in range(chunks):
            row_copy(c, k, core).wait_send()

    @pl.when(sends_halo)
    def _():
        halo_copy(0, mate).wait_send()
        halo_copy(1, tp).wait_send()

    def drain(d, carry):
        for rel in range(1 if isinstance(d, int) and d in (0, last) else CORES):
            for j in range(runs):
                if not isinstance(d, int) or d > 0:
                    ring_copy(d, rel, j).wait_send()
                mirror_out(d, rel, j).wait_send()
        return carry

    drain(0, 0)
    if full >= 1:
        drain(1, 0)
    if full >= 2:
        lax.fori_loop(2, full + 1, drain, 0)
    if last:
        drain(last, 0)


def solution(mesh):
    n = mesh.shape["sp"]
    chips = mesh.shape["tp"] // CORES
    head = 256

    def shards(*args):
        args = [a[None, :] if a.ndim == 1 else a for a in args]
        (target, source, _, _, qw, kw, _, ow, _, gw, _, _, _, dw, _) = args
        tgt_rows, width = target.shape
        r = source.shape[0]
        kv_heads = kw.shape[1] // head
        heads_here = qw.shape[1] // head
        rs = tgt_rows // (CORES * chips)
        half = chips * rs
        cols = width // 4
        chunks = width // cols
        ff = gw.shape[1]
        wide = 256 if ff % 256 == 0 else 128
        q_rows = heads_here * tgt_rows
        dists = n // 2 + 1
        sub = max(r // RUN, 1)
        runs = chips * sub
        dma = pltpu.SemaphoreType.DMA
        scratch = [pltpu.VMEM(a.shape, a.dtype) for a in args]
        scratch += [
            pltpu.VMEM((kv_heads, r, 2 * head), BF16),
            pltpu.VMEM((n * CORES * chips * r, 2 * head), BF16),
            pltpu.VMEM((q_rows, head), BF16),
            pltpu.VMEM((q_rows, 1), F32),
            pltpu.VMEM((q_rows, 1), F32),
            pltpu.VMEM((q_rows, head), F32),
            pltpu.VMEM((tgt_rows, heads_here * head), BF16),
            pltpu.VMEM((chunks, tgt_rows, cols), F32),
            pltpu.VMEM((chunks, half, cols), BF16),
            pltpu.VMEM((chunks, half, cols), BF16),
            pltpu.VMEM((chunks, half, cols), BF16),
            pltpu.VMEM((max(chips - 1, 1), chunks, half, cols), BF16),
            pltpu.VMEM((half, width), BF16),
            pltpu.VMEM((half, width), F32),
            pltpu.VMEM((chunks, tgt_rows, cols), BF16),
            pltpu.VMEM((tgt_rows, 128), F32),
            pltpu.VMEM((chunks, HALO, cols), BF16),
            pltpu.VMEM((chunks, HALO, cols), BF16),
            pltpu.VMEM((HALO + tgt_rows, ff), F32),
            pltpu.VMEM((HALO + tgt_rows, ff), F32),
            pltpu.VMEM((tgt_rows, ff), BF16),
            pltpu.VMEM((chunks, half, cols), BF16),
            pltpu.VMEM((chunks, half, cols), BF16),
            pltpu.VMEM((chunks, half, cols), BF16),
            pltpu.VMEM((max(chips - 1, 1), chunks, rs, cols), BF16),
            dma((len(args) + 2 * kv_heads,)),
            dma((runs,)),
            dma((runs,)),
        ]
        scratch += [dma((dists, CORES, runs))] * 4
        scratch += [dma((chunks,))] * 2
        scratch += [dma((chips, chunks, 2))] * 2
        scratch += [dma((chunks, chips))] * 2
        scratch += [dma((chips,))] * 2
        scratch += [dma((2,)), dma]
        scratch += [dma((chunks,))] * 2
        scratch += [dma((chips, chunks))] * 2
        return pl.pallas_call(
            functools.partial(layer, (n, chips, kv_heads, head, heads_here, cols, sub, wide)),
            out_shape=pltpu.VMEM((rs, width), BF16),
            in_specs=[pl.BlockSpec(memory_space=pl.ANY)] * len(args),
            out_specs=pl.BlockSpec(memory_space=pltpu.VMEM),
            scratch_shapes=scratch,
            compiler_params=pltpu.CompilerParams(
                collective_id=0, has_side_effects=True, vmem_limit_bytes=60 * 1024 * 1024
            ),
        )(*args)

    in_specs = (
        P("sp", None),
        P(("sp", "tp"), None),
        P(),
        P(),
        P(None, "tp"),
        P(),
        P(),
        P("tp", None),
        P(),
        P(None, "tp"),
        P(None, "tp"),
        P(None, "tp"),
        P(None, "tp"),
        P("tp", None),
        P(),
    )
    return jax.shard_map(
        shards, mesh=mesh, in_specs=in_specs, out_specs=P(("sp", "tp"), None), check_vma=False
    )
```

```python
import functools

import jax
import jax.numpy as jnp
from jax import lax
from jax.experimental import pallas as pl
from jax.experimental.pallas import tpu as pltpu
from jax.sharding import PartitionSpec as P

MESH = pl.DeviceIdType.MESH
EPS = 1e-06
HALO = 16
RUN = 32
CORES = 2
SPLIT = 8
F32 = jnp.float32
BF16 = jnp.bfloat16


def normed(values, gain):
    wide = values.astype(F32)
    scale = lax.rsqrt(jnp.mean(wide * wide, axis=-1, keepdims=True) + EPS)
    return (wide * scale * gain).astype(BF16)


def layer(
    dims,
    target_h,
    source_h,
    qgain_h,
    sgain_h,
    qw_h,
    kw_h,
    vw_h,
    ow_h,
    mgain_h,
    gw_h,
    uw_h,
    gtaps_h,
    utaps_h,
    dw_h,
    fgain_h,
    out_ref,
    tgt,
    src,
    qgain,
    sgain,
    qw,
    kw,
    vw,
    ow,
    mgain,
    gw,
    uw,
    gtaps,
    utaps,
    dw,
    fgain,
    kvh,
    kv,
    q2,
    top,
    tot,
    acc,
    att,
    chip_s,
    chip_r,
    q_held,
    res,
    rows_in,
    halo_s,
    conv_g,
    conv_u,
    hid,
    end_s,
    end_r,
    kept,
    res_s,
    res_r,
    load_sem,
    kx_s,
    kx_r,
    ring_s,
    ring_r,
    d2_s,
    d2_r,
    d2_first,
    q_s,
    q_r,
    w_s,
    w_r,
    bx_s,
    bx_r,
    h_s,
    h_r,
    r_s,
    r_r,
    fx_s,
    fx_r,
):
    n, chips, kv_heads, head, heads_here, cols, sub, wide = dims
    tgt_rows, width = tgt.shape
    r = src.shape[0]
    rs = tgt_rows // (CORES * chips)
    half_rows = chips * rs
    run = r // sub
    runs = chips * sub
    chunks = width // cols
    ff = gw_h.shape[1]
    sp = lax.axis_index("sp")
    tp = lax.axis_index("tp")
    chip = tp // CORES
    core = tp % CORES
    mate = tp + 1 - 2 * core
    base = pl.multiple_of(core * half_rows, half_rows)

    def chip_at(k):
        return (chip + k) % chips

    def ring_at(p):
        if n % 2:
            return p
        upper = p // (n // 2)
        return 2 * (p * (1 - upper) + (n - 1 - p) * upper) + upper

    if n % 2:
        pos = sp
    else:
        pos = (sp // 2) * (1 - sp % 2) + (n - 1 - sp // 2) * (sp % 2)
    ahead = ring_at((pos + 1) % n)
    behind = ring_at((pos + n - 1) % n)

    def load(index, hbm, vmem):
        copy = pltpu.make_async_copy(hbm, vmem, load_sem.at[index])
        copy.start()
        return copy

    def head_of(c):
        return (c * CORES * kv_heads) // (chips * CORES)

    own_head = head_of(chip)
    order = [(own_head + 1 + g) % kv_heads for g in range(kv_heads)]

    def columns(g):
        return pl.ds(pl.multiple_of(g * head, head), head)

    first = [load(0, source_h, src), load(1, sgain_h, sgain)]
    by_head = [
        [
            load(2 + 2 * i, kw_h.at[:, columns(g)], kw.at[:, columns(g)]),
            load(3 + 2 * i, vw_h.at[:, columns(g)], vw.at[:, columns(g)]),
        ]
        for i, g in enumerate(order)
    ]
    used = 2 + 2 * kv_heads

    barrier = pltpu.get_barrier_semaphore()
    following = (sp + 1) % n
    peers = [(ahead, tp), (behind, tp), (sp, mate)]
    peers += [(sp, chip_at(k) * CORES + core) for k in range(1, chips)]
    for peer in peers:
        pl.semaphore_signal(barrier, inc=1, device_id=peer, device_id_type=MESH)

    def remote(source_ref, dest_ref, send, recv, device):
        return pltpu.make_async_remote_copy(
            src_ref=source_ref,
            dst_ref=dest_ref,
            send_sem=send,
            recv_sem=recv,
            device_id=device,
            device_id_type=MESH,
        )

    def block(slot, lineage, j):
        start = ((slot * CORES + lineage) * runs + j) * run
        if not isinstance(start, int):
            start = pl.multiple_of(start, run)
        return kv.at[pl.ds(start, run), :]

    def chip_copy(j):
        there = chip_at(j // sub)
        return remote(
            kvh.at[head_of(there), (j % sub) * run : (j % sub + 1) * run, :],
            block(0, core, j),
            kx_s,
            kx_r.at[j - sub],
            (sp, there * CORES + core),
        )

    last = n // 2 if n % 2 == 0 else 0
    full = (n - 1) // 2
    own = range(sub)
    far = range(sub, runs)
    onward = ahead * (1 - core) + behind * core

    def slot_of(d, side):
        if isinstance(d, int) and d == 0:
            return 0
        if isinstance(d, int) and d == last:
            return n - 1
        return 2 * d - 1 + side

    def ring_copy(d, rel, j):
        lineage = core * (1 - rel) + (1 - core) * rel
        return remote(
            block(slot_of(d - 1, core), lineage, j),
            block(slot_of(d, core), lineage, j),
            ring_s,
            ring_r.at[d - 1, rel, j],
            (onward, tp),
        )

    def mirror_copy(d, rel, j, side):
        lineage = side * (1 - rel) + (1 - side) * rel
        held = block(slot_of(d, side), lineage, j)
        first = isinstance(d, int) and d == 0
        return remote(held, held, d2_s, d2_first.at[j] if first else d2_r.at[d - 1], (sp, mate))

    def mirror_out(d, rel, j):
        return mirror_copy(d, rel, j, core)

    def mirror_in(d, rel, j):
        return mirror_copy(d, rel, j, 1 - core)

    def whole(w, side):
        high = w.shape[0] // CORES
        return w.at[pl.ds(pl.multiple_of(side * high, high), high), :]

    shared = [
        (ow_h, lambda side: whole(ow, side), SPLIT),
        (gw_h, lambda side: gw.at[side], SPLIT),
        (uw_h, lambda side: uw.at[side], SPLIT),
        (gtaps_h, lambda side: gtaps.at[side], 1),
        (utaps_h, lambda side: utaps.at[side], 1),
        (dw_h, lambda side: whole(dw, side), SPLIT),
    ]

    def push(i, p, side):
        held, place, pieces = shared[i]
        high = held.shape[0] // pieces
        at = slice(p * high, (p + 1) * high)
        there = place(side)
        return remote(
            held.at[at, :], there.at[at, :], w_s.at[i], w_r.at[i], (sp, mate)
        )

    def pushed(i, side):
        held, place, _ = shared[i]
        return remote(held, place(side), w_s.at[i], w_r.at[i], (sp, mate))

    pending = [(i, p) for i in range(len(shared)) for p in range(shared[i][2])]

    def feed(count):
        for x in pending[:count]:
            push(*x, core).start()
        del pending[:count]

    def shared_wait(i):
        pushed(i, 1 - core).wait_recv()

    def launch(j):
        if n > 1:
            ring_copy(1, 0, j).start()
        mirror_out(0, 0, j).start()

    def launch_mate(blocks):
        for j in blocks:
            mirror_in(0, 0, j).wait_recv()
            if full >= 1:
                ring_copy(1, 1, j).start()

    def launch_far():
        for j in far:
            chip_copy(j).wait_recv()
            launch(j)

    quota = {1: 5, 2: 4, 3: 3}

    def arrive(d, rel, blocks):
        end = isinstance(d, int) and d == full
        for j in blocks:
            ring_copy(d, rel, j).wait_recv()
            if not end or (last and rel == 0):
                ring_copy(d + 1, rel, j).start()
            mirror_out(d, rel, j).start()
            if isinstance(d, int) and d in quota and quota[d] > 0:
                quota[d] -= 1
                feed(1)

    def arrive_last(blocks):
        if last:
            for j in blocks:
                ring_copy(last, 0, j).wait_recv()
                mirror_out(last, 0, j).start()

    for copy in first:
        copy.wait()
    source_in = normed(src[...], sgain[...])
    second = [
        load(used + i, a, b)
        for i, (a, b) in enumerate(((target_h, tgt), (qgain_h, qgain), (qw_h, qw)))
    ]
    early = chips == kv_heads
    for i, g in enumerate(order):
        for copy in by_head[i]:
            copy.wait()
        keys = jnp.dot(source_in, kw[:, columns(g)], preferred_element_type=F32)
        kvh[g, :, :head] = keys.astype(BF16)
        values = jnp.dot(source_in, vw[:, columns(g)], preferred_element_type=F32)
        kvh[g, :, head:] = values.astype(BF16)
        if i == (kv_heads - 2 if early else kv_heads - 1):
            pl.semaphore_wait(barrier, len(peers))
            for j in range(sub, runs):
                chip_copy(j).start()
    kv[pl.ds(pl.multiple_of(core * chips * r, r), r), :] = kvh[own_head]
    for j in range(sub):
        launch(j)
    for copy in second:
        copy.wait()
    queries = jnp.dot(normed(tgt[...], qgain[...]), qw[...], preferred_element_type=F32).astype(
        BF16
    )
    group = heads_here * half_rows
    for side in range(CORES):
        for h in range(heads_here):
            q_held[side, h * half_rows : (h + 1) * half_rows, :] = queries[
                side * half_rows : (side + 1) * half_rows, h * head : (h + 1) * head
            ]

    def q_copy(side):
        return remote(
            q_held.at[1 - core],
            q2.at[pl.ds(pl.multiple_of(side * group, group), group), :],
            q_s,
            q_r,
            (sp, mate),
        )

    q_copy(core).start()
    q2[pl.ds(pl.multiple_of(core * group, group), group), :] = q_held[core]
    top[...] = jnp.full(top.shape, -1e30, F32)
    tot[...] = jnp.zeros(tot.shape, F32)
    acc[...] = jnp.zeros(acc.shape, F32)

    slot_rows = CORES * chips * r

    def attend(slot, slots):
        start = slot * slot_rows
        if not isinstance(start, int):
            start = pl.multiple_of(start, slot_rows)
        here = pl.ds(start, slots * slot_rows)
        scores = lax.dot_general(
            q2[...], kv[here, :head], (((1,), (1,)), ((), ())), preferred_element_type=F32
        ) * (head**-0.5)
        old = top[...]
        new = jnp.maximum(old, jnp.max(scores, axis=-1, keepdims=True))
        shrink = jnp.exp(old - new)
        probs = jnp.exp(scores - new)
        top[...] = new
        tot[...] = tot[...] * shrink + jnp.sum(probs, axis=-1, keepdims=True)
        acc[...] = acc[...] * shrink + jnp.dot(
            probs.astype(BF16), kv[here, head:], preferred_element_type=F32
        )

    def local_loads():
        pairs = [(held, place(core)) for held, place, _ in shared]
        pairs += [(mgain_h, mgain), (fgain_h, fgain)]
        return [load(used + 3 + i, a, b) for i, (a, b) in enumerate(pairs)]

    def mirrored(d):
        end = isinstance(d, int) and d == last
        rows = slot_rows // CORES if end else slot_rows
        start = slot_of(d, 1 - core) * slot_rows
        if end:
            start = start + (1 - core) * rows
        held = kv.at[pl.ds(pl.multiple_of(start, rows), rows), :]
        remote(held, held, d2_s, d2_r.at[d - 1], (sp, mate)).wait_recv()

    def wave(d):
        for blocks in (own, far):
            for rel in range(CORES):
                arrive(d, rel, blocks)

    if full >= 1:
        feed(2)
        launch_mate(own)
        launch_far()
        feed(3)
        launch_mate(far)
        q_copy(1 - core).wait_recv()
        wave(1)
        rest = local_loads()
        done = 1
        if full > 4:
            wave(2)
            attend(0, 1)

            def middle(d, carry):
                wave(d)
                mirrored(d - 2)
                attend(2 * d - 5, 2)
                return carry

            lax.fori_loop(3, full, middle, 0)
            wave(full)
            done = full - 2
        else:
            for d in range(2, full + 1):
                wave(d)
        start = 2 * done - 1 if full > 4 else 0
        for d in range(done, full):
            mirrored(d)
        attend(start, 2 * full - 1 - start)
        arrive_last(range(runs))
        feed(len(pending) - SPLIT)
        mirrored(full)
        attend(2 * full - 1, 2)
    else:
        rest = local_loads()
        launch_far()
        launch_mate(range(runs))
        q_copy(1 - core).wait_recv()
        arrive_last(range(runs))
        feed(3 * SPLIT + 2)
        attend(0, 1)
    if last:
        mirrored(last)
        attend(n - 1, 1)

    attended = (acc[...] / tot[...]).astype(BF16)
    for h in range(CORES * heads_here):
        att[:, h * head : (h + 1) * head] = attended[h * half_rows : (h + 1) * half_rows, :]
    for copy in rest:
        copy.wait()
    shared_wait(0)

    body_rows = half_rows - HALO
    body = slice(0, body_rows)
    tail = slice(body_rows, half_rows)

    def wide_copy(k, c, i):
        at = (body, tail)[i]
        return remote(
            chip_s.at[c, at, :],
            chip_r.at[k - 1, c, at, :],
            bx_s.at[k],
            bx_r.at[k, c * (1 - i) + chunks * i],
            (sp, chip_at(k) * CORES + core),
        )

    for c in range(chunks):
        here = slice(c * cols, (c + 1) * cols)
        product = jnp.dot(att[...], ow[:, here], preferred_element_type=F32)
        chip_s[c] = product.astype(BF16)
        for k in range(1, chips):
            wide_copy(k, c, 1).start()
        res[:, here] = product + tgt[pl.ds(base, half_rows), here].astype(F32)
    for c in range(chunks):
        for k in range(1, chips):
            wide_copy(k, c, 0).start()

    def wide_all(k, at, recv):
        return remote(
            chip_s.at[:, at, :],
            chip_r.at[k - 1, :, at, :],
            bx_s.at[k],
            bx_r.at[k, recv],
            (sp, chip_at(k) * CORES + core),
        )

    def settle(c, i):
        at = (body, tail)[i]
        here = slice(c * cols, (c + 1) * cols)
        residual = res[at, here]
        for k in range(1, chips):
            if i == 0:
                wide_copy(k, c, 0).wait_recv()
            residual = residual + chip_r[k - 1, c, at, :].astype(F32)
        residual = residual.astype(BF16).astype(F32)
        res[at, here] = residual
        return jnp.sum(residual * residual, axis=-1, keepdims=True)

    for k in range(1, chips):
        wide_all(k, tail, chunks).wait_recv()

    beyond = sp * (1 - core) + following * core

    halo = remote(halo_s, rows_in.at[:, 0:HALO, :], h_s, h_r, (beyond, mate))

    sends_halo = jnp.logical_or(core == 0, sp < n - 1)
    takes_halo = jnp.logical_or(core == 1, sp > 0)
    tail_squares = settle(0, 1)
    for c in range(1, chunks):
        tail_squares = tail_squares + settle(c, 1)
    scale = lax.rsqrt(tail_squares / width + EPS)
    for c in range(chunks):
        here = slice(c * cols, (c + 1) * cols)
        halo_s[c] = (res[tail, here] * scale * mgain[:, here]).astype(BF16)

    @pl.when(sends_halo)
    def _():
        halo.start()

    feed(len(pending))

    @pl.when(jnp.logical_not(takes_halo))
    def _():
        rows_in[:, 0:HALO, :] = jnp.zeros((chunks, HALO, cols), BF16)

    def ready():
        @pl.when(takes_halo)
        def _():
            halo.wait_recv()

    def mix(c):
        here = slice(c * cols, (c + 1) * cols)
        for side in range(CORES):
            there = slice(side * ff, (side + 1) * ff)
            for weight, total in ((gw, conv_g), (uw, conv_u)):
                product = jnp.dot(
                    rows_in[c], weight[side, here, :], preferred_element_type=F32
                )
                if c > 0:
                    product = product + total[:, there]
                total[:, there] = product

    for i in range(1, len(shared) - 1):
        shared_wait(i)
    squares = jnp.zeros((body_rows, 1), F32)
    for c in range(chunks):
        squares = squares + settle(c, 0)
        here = slice(c * cols, (c + 1) * cols)
        rows_in[c, HALO:, :] = (res[:, here] * mgain[:, here]).astype(BF16)
        if c == chunks - 2:
            ready()
            for i in range(chunks - 1):
                mix(i)
    squares = jnp.concatenate([squares, tail_squares], axis=0)
    scale = jnp.concatenate(
        [jnp.ones((HALO, 1), F32), lax.rsqrt(squares / width + EPS)], axis=0
    )

    from_core = tp // chips
    held_row = pl.multiple_of((tp % chips) * rs, rs)
    mate_row = pl.multiple_of((mate % chips) * rs, rs)
    sends_res = mate // chips == core
    holds = from_core == core

    def res_copy():
        return remote(res_s, res_r, r_s, r_r, (sp, mate))

    @pl.when(sends_res)
    def _():
        res_s[...] = res[pl.ds(mate_row, rs), :].astype(BF16)
        res_copy().start()

    taps = gtaps.shape[1]
    last_rows = slice((chunks - 1) * cols, chunks * cols)
    blocks_here = ff // wide
    for f in range(CORES * blocks_here):
        side = f // blocks_here
        part = slice((f % blocks_here) * wide, (f % blocks_here + 1) * wide)
        here = slice(f * wide, (f + 1) * wide)
        for weight, total in ((gw, conv_g), (uw, conv_u)):
            product = total[:, here] + jnp.dot(
                rows_in[chunks - 1], weight[side, last_rows, part], preferred_element_type=F32
            )
            total[:, here] = (product * scale).astype(BF16).astype(F32)
        gate = jnp.zeros((half_rows, wide), F32)
        up = jnp.zeros((half_rows, wide), F32)
        for t in range(taps):
            begin = HALO - (taps - 1) + t
            rows = slice(begin, begin + half_rows)
            gate = gate + gtaps[side, t : t + 1, part].astype(F32) * conv_g[rows, here]
            up = up + utaps[side, t : t + 1, part].astype(F32) * conv_u[rows, here]
        hid[:, here] = (gate / (1.0 + jnp.exp(-gate)) * up).astype(BF16)

    @pl.when(holds)
    def _():
        end_r[chip] = jnp.zeros(end_r.shape[1:], BF16)

    @pl.when(jnp.logical_not(holds))
    def _():
        kept[...] = jnp.zeros(kept.shape, F32)

    shared_wait(len(shared) - 1)

    def end_copy(i, c):
        there = core * chips + i
        return remote(
            end_s.at[c, i * rs : (i + 1) * rs, :],
            end_r.at[chip, c],
            fx_s.at[i],
            fx_r.at[chip, c // (chunks - 1)],
            (sp, there),
        )

    def end_in(k, i):
        at = slice(0, chunks - 1) if i == 0 else slice(chunks - 1, chunks)
        return remote(
            end_s.at[at, 0:rs, :], end_r.at[k, at], fx_s.at[0], fx_r.at[k, i], (sp, mate)
        )

    def end_out(i):
        held = end_s.at[:, i * rs : (i + 1) * rs, :]
        return remote(held, end_r.at[chip], fx_s.at[i], fx_r.at[chip, 0], (sp, mate))

    for c in range(chunks):
        here = slice(c * cols, (c + 1) * cols)
        product = jnp.dot(hid[...], dw[:, here], preferred_element_type=F32)
        end_s[c] = product.astype(BF16)
        for i in range(chips):

            @pl.when(core * chips + i != tp)
            def _(i=i, c=c):
                end_copy(i, c).start()

            @pl.when(core * chips + i == tp)
            def _(i=i, here=here, product=product):
                kept[:, here] = product[i * rs : (i + 1) * rs, :]

    @pl.when(holds)
    def _():
        kept[...] = kept[...] + res[pl.ds(held_row, rs), :]

    @pl.when(jnp.logical_not(holds))
    def _():
        res_copy().wait_recv()
        kept[...] = res_r[...].astype(F32)

    squares = jnp.zeros((rs, 1), F32)
    sums = []
    for c in range(chunks):
        here = slice(c * cols, (c + 1) * cols)
        if c in (0, chunks - 1):
            for k in range(chips):

                @pl.when(k * CORES + from_core != tp)
                def _(k=k, c=c):
                    end_in(k, c // (chunks - 1)).wait_recv()

        total = kept[:, here]
        for k in range(chips):
            total = total + end_r[k, c].astype(F32)
        squares = squares + jnp.sum(total * total, axis=-1, keepdims=True)
        sums.append(total)
    scale = lax.rsqrt(squares / width + EPS)
    for c in range(chunks):
        here = slice(c * cols, (c + 1) * cols)
        out_ref[:, here] = (sums[c] * scale * fgain[:, here]).astype(BF16)

    def sent(rows, sem):
        held = kv.at[0:rows, :]
        remote(held, held, sem, d2_r.at[0], (sp, mate)).wait_send()

    if chips > 1:
        sent((chips - 1) * r, kx_s)
    q_copy(core).wait_send()
    for i in range(len(shared)):
        pushed(i, core).wait_send()
    for k in range(1, chips):
        wide_all(k, slice(0, half_rows), chunks).wait_send()
    for i in range(chips):

        @pl.when(core * chips + i != tp)
        def _(i=i):
            end_out(i).wait_send()

    @pl.when(sends_halo)
    def _():
        halo.wait_send()

    @pl.when(sends_res)
    def _():
        res_copy().wait_send()

    sent(n * runs * run, d2_s)
    if n > 1:
        sent((full * CORES + (1 if last else 0)) * runs * run, ring_s)


def solution(mesh):
    n = mesh.shape["sp"]
    chips = mesh.shape["tp"] // CORES
    head = 256

    def shards(*args):
        args = [a[None, :] if a.ndim == 1 else a for a in args]
        (target, source, _, _, qw, kw, _, ow, _, gw, _, _, _, dw, _) = args
        tgt_rows, width = target.shape
        r = source.shape[0]
        kv_heads = kw.shape[1] // head
        heads_here = qw.shape[1] // head
        rs = tgt_rows // (CORES * chips)
        half = chips * rs
        cols = width // 4
        chunks = width // cols
        ff = gw.shape[1]
        wide = 256 if ff % 256 == 0 else 128
        q_rows = heads_here * tgt_rows
        sub = max(r // RUN, 1)
        runs = chips * sub
        dma = pltpu.SemaphoreType.DMA
        shapes = [a.shape for a in args]
        for i in (9, 10, 11, 12):
            shapes[i] = (CORES,) + shapes[i]
        for i in (7, 13):
            shapes[i] = (CORES * shapes[i][0], shapes[i][1])
        scratch = [pltpu.VMEM(shape, a.dtype) for shape, a in zip(shapes, args, strict=True)]
        scratch += [
            pltpu.VMEM((kv_heads, r, 2 * head), BF16),
            pltpu.VMEM((n * CORES * chips * r, 2 * head), BF16),
            pltpu.VMEM((q_rows, head), BF16),
            pltpu.VMEM((q_rows, 1), F32),
            pltpu.VMEM((q_rows, 1), F32),
            pltpu.VMEM((q_rows, head), F32),
            pltpu.VMEM((half, CORES * heads_here * head), BF16),
            pltpu.VMEM((chunks, half, cols), BF16),
            pltpu.VMEM((max(chips - 1, 1), chunks, half, cols), BF16),
            pltpu.VMEM((CORES, heads_here * half, head), BF16),
            pltpu.VMEM((half, width), F32),
            pltpu.VMEM((chunks, HALO + half, cols), BF16),
            pltpu.VMEM((chunks, HALO, cols), BF16),
            pltpu.VMEM((HALO + half, CORES * ff), F32),
            pltpu.VMEM((HALO + half, CORES * ff), F32),
            pltpu.VMEM((half, CORES * ff), BF16),
            pltpu.VMEM((chunks, half, cols), BF16),
            pltpu.VMEM((chips, chunks, rs, cols), BF16),
            pltpu.VMEM((rs, width), F32),
            pltpu.VMEM((rs, width), BF16),
            pltpu.VMEM((rs, width), BF16),
            dma((len(args) + 2 * kv_heads,)),
            dma,
            dma((max(runs - sub, 1),)),
            dma,
            dma((max(n // 2, 1), CORES, runs)),
            dma,
            dma((max(n // 2, 1),)),
            dma((runs,)),
        ]
        scratch += [dma] * 2
        scratch += [dma((6,))] * 2
        scratch += [dma((chips,)), dma((chips, chunks + 1))]
        scratch += [dma] * 4
        scratch += [dma((chips,)), dma((chips, 2))]
        return pl.pallas_call(
            functools.partial(layer, (n, chips, kv_heads, head, heads_here, cols, sub, wide)),
            out_shape=pltpu.VMEM((rs, width), BF16),
            in_specs=[pl.BlockSpec(memory_space=pl.ANY)] * len(args),
            out_specs=pl.BlockSpec(memory_space=pltpu.VMEM),
            scratch_shapes=scratch,
            compiler_params=pltpu.CompilerParams(
                collective_id=0, has_side_effects=True, vmem_limit_bytes=60 * 1024 * 1024
            ),
        )(*args)

    in_specs = (
        P("sp", None),
        P(("sp", "tp"), None),
        P(),
        P(),
        P(None, "tp"),
        P(),
        P(),
        P("tp", None),
        P(),
        P(None, "tp"),
        P(None, "tp"),
        P(None, "tp"),
        P(None, "tp"),
        P("tp", None),
        P(),
    )
    return jax.shard_map(
        shards, mesh=mesh, in_specs=in_specs, out_specs=P(("sp", "tp"), None), check_vma=False
    )
```

```python
import functools

import jax
import jax.numpy as jnp
from jax import lax
from jax.experimental import pallas as pl
from jax.experimental.pallas import tpu as pltpu
from jax.sharding import PartitionSpec as P

MESH = pl.DeviceIdType.MESH
EPS = 1e-06
HALO = 16
RUN = 32
CORES = 2
SPLIT = 8
F32 = jnp.float32
BF16 = jnp.bfloat16


def normed(values, gain):
    wide = values.astype(F32)
    scale = lax.rsqrt(jnp.mean(wide * wide, axis=-1, keepdims=True) + EPS)
    return (wide * scale * gain).astype(BF16)


def layer(
    dims,
    target_h,
    source_h,
    qgain_h,
    sgain_h,
    qw_h,
    kw_h,
    vw_h,
    ow_h,
    mgain_h,
    gw_h,
    uw_h,
    gtaps_h,
    utaps_h,
    dw_h,
    fgain_h,
    out_ref,
    tgt,
    src,
    qgain,
    sgain,
    qw,
    kw,
    vw,
    ow,
    mgain,
    gw,
    uw,
    gtaps,
    utaps,
    dw,
    fgain,
    kvh,
    kv,
    q2,
    top,
    tot,
    acc,
    att,
    chip_s,
    chip_r,
    q_held,
    res,
    rows_in,
    halo_s,
    conv_g,
    conv_u,
    hid,
    end_s,
    end_r,
    kept,
    res_s,
    res_r,
    load_sem,
    kx_s,
    kx_r,
    ring_s,
    ring_r,
    d2_s,
    d2_r,
    d2_first,
    q_s,
    q_r,
    w_s,
    w_r,
    bx_s,
    bx_r,
    h_s,
    h_r,
    r_s,
    r_r,
    fx_s,
    fx_r,
):
    n, chips, kv_heads, head, heads_here, cols, sub, wide = dims
    tgt_rows, width = tgt.shape
    r = src.shape[0]
    rs = tgt_rows // (CORES * chips)
    half_rows = chips * rs
    run = r // sub
    runs = chips * sub
    chunks = width // cols
    ff = gw_h.shape[1]
    sp = lax.axis_index("sp")
    tp = lax.axis_index("tp")
    chip = tp // CORES
    core = tp % CORES
    mate = tp + 1 - 2 * core
    span = (core + chip) % CORES
    base = pl.multiple_of(span * half_rows, half_rows)

    def chip_at(k):
        return (chip + k) % chips

    def ring_at(p):
        if n % 2:
            return p
        upper = p // (n // 2)
        return 2 * (p * (1 - upper) + (n - 1 - p) * upper) + upper

    if n % 2:
        pos = sp
    else:
        pos = (sp // 2) * (1 - sp % 2) + (n - 1 - sp // 2) * (sp % 2)
    ahead = ring_at((pos + 1) % n)
    behind = ring_at((pos + n - 1) % n)

    def load(index, hbm, vmem):
        copy = pltpu.make_async_copy(hbm, vmem, load_sem.at[index])
        copy.start()
        return copy

    def head_of(c):
        return (c * CORES * kv_heads) // (chips * CORES)

    own_head = head_of(chip)
    order = [(own_head + 1 + g) % kv_heads for g in range(kv_heads)]

    def columns(g):
        return pl.ds(pl.multiple_of(g * head, head), head)

    first = [load(0, source_h, src), load(1, sgain_h, sgain)]
    by_head = [
        [
            load(2 + 2 * i, kw_h.at[:, columns(g)], kw.at[:, columns(g)]),
            load(3 + 2 * i, vw_h.at[:, columns(g)], vw.at[:, columns(g)]),
        ]
        for i, g in enumerate(order)
    ]
    used = 2 + 2 * kv_heads

    barrier = pltpu.get_barrier_semaphore()
    following = (sp + 1) % n
    peers = [(ahead, tp), (behind, tp), (sp, mate)]
    peers += [(sp, chip_at(k) * CORES + i) for k in range(1, chips) for i in range(CORES)]
    for peer in peers:
        pl.semaphore_signal(barrier, inc=1, device_id=peer, device_id_type=MESH)

    def remote(source_ref, dest_ref, send, recv, device):
        return pltpu.make_async_remote_copy(
            src_ref=source_ref,
            dst_ref=dest_ref,
            send_sem=send,
            recv_sem=recv,
            device_id=device,
            device_id_type=MESH,
        )

    def block(slot, lineage, j):
        start = ((slot * CORES + lineage) * runs + j) * run
        if not isinstance(start, int):
            start = pl.multiple_of(start, run)
        return kv.at[pl.ds(start, run), :]

    def chip_copy(j):
        there = chip_at(j // sub)
        return remote(
            kvh.at[head_of(there), (j % sub) * run : (j % sub + 1) * run, :],
            block(0, core, j),
            kx_s,
            kx_r.at[j - sub],
            (sp, there * CORES + core),
        )

    last = n // 2 if n % 2 == 0 else 0
    full = (n - 1) // 2
    own = range(sub)
    far = range(sub, runs)
    onward = ahead * (1 - core) + behind * core

    def slot_of(d, side):
        if isinstance(d, int) and d == 0:
            return 0
        if isinstance(d, int) and d == last:
            return n - 1
        return 2 * d - 1 + side

    def ring_copy(d, rel, j):
        lineage = core * (1 - rel) + (1 - core) * rel
        return remote(
            block(slot_of(d - 1, core), lineage, j),
            block(slot_of(d, core), lineage, j),
            ring_s,
            ring_r.at[d - 1, rel, j],
            (onward, tp),
        )

    def mirror_copy(d, rel, j, side):
        lineage = side * (1 - rel) + (1 - side) * rel
        held = block(slot_of(d, side), lineage, j)
        first = isinstance(d, int) and d == 0
        return remote(held, held, d2_s, d2_first.at[j] if first else d2_r.at[d - 1], (sp, mate))

    def mirror_out(d, rel, j):
        return mirror_copy(d, rel, j, core)

    def mirror_in(d, rel, j):
        return mirror_copy(d, rel, j, 1 - core)

    def whole(w, side):
        high = w.shape[0] // CORES
        return w.at[pl.ds(pl.multiple_of(side * high, high), high), :]

    shared = [
        (ow_h, lambda side: whole(ow, side), SPLIT),
        (gw_h, lambda side: gw.at[side], SPLIT),
        (uw_h, lambda side: uw.at[side], SPLIT),
        (gtaps_h, lambda side: gtaps.at[side], 1),
        (utaps_h, lambda side: utaps.at[side], 1),
        (dw_h, lambda side: whole(dw, side), SPLIT),
    ]

    def push(i, p, side):
        held, place, pieces = shared[i]
        high = held.shape[0] // pieces
        at = slice(p * high, (p + 1) * high)
        there = place(side)
        return remote(
            held.at[at, :], there.at[at, :], w_s.at[i], w_r.at[i], (sp, mate)
        )

    def pushed(i, side):
        held, place, _ = shared[i]
        return remote(held, place(side), w_s.at[i], w_r.at[i], (sp, mate))

    pending = [(i, p) for i in range(len(shared)) for p in range(shared[i][2])]

    def feed(count):
        for x in pending[:count]:
            push(*x, core).start()
        del pending[:count]

    def shared_wait(i):
        pushed(i, 1 - core).wait_recv()

    def launch(j):
        if full >= 1 or (last and (0, j) in ends):
            ring_copy(1, 0, j).start()
        elif last:

            @pl.when(core == 1)
            def _():
                ring_copy(1, 0, j).start()

        mirror_out(0, 0, j).start()

    def launch_mate(blocks):
        for j in blocks:
            mirror_in(0, 0, j).wait_recv()
            if full >= 1:
                ring_copy(1, 1, j).start()
            elif last and (1, j) in more:

                @pl.when(core == 1)
                def _(j=j):
                    ring_copy(1, 1, j).start()

    def launch_far():
        for j in far:
            chip_copy(j).wait_recv()
            launch(j)

    quota = {1: 6, 2: 5, 3: 1}
    ends = [(0, j) for j in own]
    more = [(rel, j) for rel in range(CORES) for j in far]

    def arrive(d, rel, blocks):
        end = isinstance(d, int) and d == full
        for j in blocks:
            ring_copy(d, rel, j).wait_recv()
            if not end or (last and (rel, j) in ends):
                ring_copy(d + 1, rel, j).start()
            elif last and (rel, j) in more:

                @pl.when(core == 1)
                def _(rel=rel, j=j):
                    ring_copy(last, rel, j).start()

            mirror_out(d, rel, j).start()
            if isinstance(d, int) and d in quota and quota[d] > 0:
                quota[d] -= 1
                feed(1)

    def arrive_last():
        if last:
            for rel, j in ends:
                ring_copy(last, rel, j).wait_recv()
                mirror_out(last, rel, j).start()

            if more:

                @pl.when(core == 1)
                def _():
                    for rel, j in more:
                        ring_copy(last, rel, j).wait_recv()
                        mirror_out(last, rel, j).start()

    for copy in first:
        copy.wait()
    source_in = normed(src[...], sgain[...])
    second = [
        load(used + i, a, b)
        for i, (a, b) in enumerate(((target_h, tgt), (qgain_h, qgain), (qw_h, qw)))
    ]
    early = chips == kv_heads
    for i, g in enumerate(order):
        for copy in by_head[i]:
            copy.wait()
        keys = jnp.dot(source_in, kw[:, columns(g)], preferred_element_type=F32)
        kvh[g, :, :head] = keys.astype(BF16)
        values = jnp.dot(source_in, vw[:, columns(g)], preferred_element_type=F32)
        kvh[g, :, head:] = values.astype(BF16)
        if i == (kv_heads - 2 if early else kv_heads - 1):
            pl.semaphore_wait(barrier, len(peers))
            for j in range(sub, runs):
                chip_copy(j).start()
    kv[pl.ds(pl.multiple_of(core * chips * r, r), r), :] = kvh[own_head]
    for j in range(sub):
        launch(j)
    for copy in second:
        copy.wait()
    queries = jnp.dot(normed(tgt[...], qgain[...]), qw[...], preferred_element_type=F32).astype(
        BF16
    )
    group = heads_here * half_rows
    for side in range(CORES):
        for h in range(heads_here):
            q_held[side, h * half_rows : (h + 1) * half_rows, :] = queries[
                side * half_rows : (side + 1) * half_rows, h * head : (h + 1) * head
            ]

    def q_copy(side):
        return remote(
            q_held.at[1 - span],
            q2.at[pl.ds(pl.multiple_of(side * group, group), group), :],
            q_s,
            q_r,
            (sp, mate),
        )

    q_copy(core).start()
    q2[pl.ds(pl.multiple_of(core * group, group), group), :] = q_held[span]
    top[...] = jnp.full(top.shape, -1e30, F32)
    tot[...] = jnp.zeros(tot.shape, F32)
    acc[...] = jnp.zeros(acc.shape, F32)

    slot_rows = CORES * chips * r

    def attend(slot, slots):
        start = slot * slot_rows
        if not isinstance(start, int):
            start = pl.multiple_of(start, slot_rows)
        here = pl.ds(start, slots * slot_rows)
        scores = lax.dot_general(
            q2[...], kv[here, :head], (((1,), (1,)), ((), ())), preferred_element_type=F32
        ) * (head**-0.5)
        old = top[...]
        new = jnp.maximum(old, jnp.max(scores, axis=-1, keepdims=True))
        shrink = jnp.exp(old - new)
        probs = jnp.exp(scores - new)
        top[...] = new
        tot[...] = tot[...] * shrink + jnp.sum(probs, axis=-1, keepdims=True)
        acc[...] = acc[...] * shrink + jnp.dot(
            probs.astype(BF16), kv[here, head:], preferred_element_type=F32
        )

    def local_loads():
        pairs = [(held, place(core)) for held, place, _ in shared]
        pairs += [(mgain_h, mgain), (fgain_h, fgain)]
        return [load(used + 3 + i, a, b) for i, (a, b) in enumerate(pairs)]

    def mirror_wait(d, start, rows):
        held = kv.at[pl.ds(start, rows), :]
        remote(held, held, d2_s, d2_r.at[d - 1], (sp, mate)).wait_recv()

    def mirrored(d):
        if isinstance(d, int) and d == last:
            begin = (n - 1) * slot_rows

            @pl.when(core == 1)
            def _():
                mirror_wait(d, begin, len(ends) * run)

            if more:

                @pl.when(core == 0)
                def _():
                    mirror_wait(d, begin + len(ends) * run, slot_rows - len(ends) * run)
        else:
            start = slot_of(d, 1 - core) * slot_rows
            mirror_wait(d, pl.multiple_of(start, slot_rows), slot_rows)

    def wave(d):
        for blocks in (own, far):
            for rel in range(CORES):
                arrive(d, rel, blocks)

    if full >= 1:
        feed(4)
        launch_mate(own)
        launch_far()
        feed(3)
        launch_mate(far)
        q_copy(1 - core).wait_recv()
        wave(1)
        rest = local_loads()
        done = 1
        if full > 4:
            wave(2)
            attend(0, 1)

            def middle(d, carry):
                wave(d)
                mirrored(d - 2)
                attend(2 * d - 5, 2)
                return carry

            lax.fori_loop(3, full, middle, 0)
            wave(full)
            done = full - 2
        else:
            for d in range(2, full + 1):
                wave(d)
        start = 2 * done - 1 if full > 4 else 0
        for d in range(done, full):
            mirrored(d)
        attend(start, 2 * full - 1 - start)
        arrive_last()
        feed(len(pending) - SPLIT // 2)
        mirrored(full)
        attend(2 * full - 1, 2)
    else:
        rest = local_loads()
        launch_far()
        launch_mate(range(runs))
        q_copy(1 - core).wait_recv()
        arrive_last()
        feed(3 * SPLIT + 2)
        attend(0, 1)
    if last:
        mirrored(last)
        attend(n - 1, 1)

    attended = (acc[...] / tot[...]).astype(BF16)
    for h in range(CORES * heads_here):
        att[:, h * head : (h + 1) * head] = attended[h * half_rows : (h + 1) * half_rows, :]
    for copy in rest:
        copy.wait()
    shared_wait(0)

    body_rows = half_rows - HALO
    body = slice(0, body_rows)
    tail = slice(body_rows, half_rows)

    def peer_of(k):
        there = chip_at(k)
        return there * CORES + (span + there) % CORES

    def wide_copy(k, c, i):
        at = (body, tail)[i]
        return remote(
            chip_s.at[c, at, :],
            chip_r.at[k - 1, c, at, :],
            bx_s.at[k],
            bx_r.at[k, c * (1 - i) + chunks * i],
            (sp, peer_of(k)),
        )

    for c in range(chunks):
        here = slice(c * cols, (c + 1) * cols)
        product = jnp.dot(att[...], ow[:, here], preferred_element_type=F32)
        chip_s[c] = product.astype(BF16)
        for k in range(1, chips):
            wide_copy(k, c, 1).start()
        res[:, here] = product + tgt[pl.ds(base, half_rows), here].astype(F32)
    for c in range(chunks):
        for k in range(1, chips):
            wide_copy(k, c, 0).start()

    def wide_all(k, at, recv):
        return remote(
            chip_s.at[:, at, :],
            chip_r.at[k - 1, :, at, :],
            bx_s.at[k],
            bx_r.at[k, recv],
            (sp, peer_of(k)),
        )

    def settle(c, i):
        at = (body, tail)[i]
        here = slice(c * cols, (c + 1) * cols)
        residual = res[at, here]
        for k in range(1, chips):
            if i == 0:
                wide_copy(k, c, 0).wait_recv()
            residual = residual + chip_r[k - 1, c, at, :].astype(F32)
        residual = residual.astype(BF16).astype(F32)
        res[at, here] = residual
        return jnp.sum(residual * residual, axis=-1, keepdims=True)

    for k in range(1, chips):
        wide_all(k, tail, chunks).wait_recv()

    beyond = sp * (1 - span) + following * span

    halo = remote(halo_s, rows_in.at[:, 0:HALO, :], h_s, h_r, (beyond, mate))

    sends_halo = jnp.logical_or(span == 0, sp < n - 1)
    takes_halo = jnp.logical_or(span == 1, sp > 0)
    tail_squares = settle(0, 1)
    for c in range(1, chunks):
        tail_squares = tail_squares + settle(c, 1)
    scale = lax.rsqrt(tail_squares / width + EPS)
    for c in range(chunks):
        here = slice(c * cols, (c + 1) * cols)
        halo_s[c] = (res[tail, here] * scale * mgain[:, here]).astype(BF16)

    @pl.when(sends_halo)
    def _():
        halo.start()

    feed(len(pending))

    @pl.when(jnp.logical_not(takes_halo))
    def _():
        rows_in[:, 0:HALO, :] = jnp.zeros((chunks, HALO, cols), BF16)

    def ready():
        @pl.when(takes_halo)
        def _():
            halo.wait_recv()

    def mix(c):
        here = slice(c * cols, (c + 1) * cols)
        for side in range(CORES):
            there = slice(side * ff, (side + 1) * ff)
            for weight, total in ((gw, conv_g), (uw, conv_u)):
                product = jnp.dot(
                    rows_in[c], weight[side, here, :], preferred_element_type=F32
                )
                if c > 0:
                    product = product + total[:, there]
                total[:, there] = product

    for i in range(1, len(shared) - 1):
        shared_wait(i)
    squares = jnp.zeros((body_rows, 1), F32)
    for c in range(chunks):
        squares = squares + settle(c, 0)
        here = slice(c * cols, (c + 1) * cols)
        rows_in[c, HALO:, :] = (res[:, here] * mgain[:, here]).astype(BF16)
        if c == 1:
            ready()
            mix(0)
        elif c == chunks - 2:
            for i in range(1, chunks - 1):
                mix(i)
    squares = jnp.concatenate([squares, tail_squares], axis=0)
    scale = jnp.concatenate(
        [jnp.ones((HALO, 1), F32), lax.rsqrt(squares / width + EPS)], axis=0
    )

    source = tp // chips
    held_row = pl.multiple_of((tp % chips) * rs, rs)
    mate_row = pl.multiple_of((mate % chips) * rs, rs)
    sends_res = mate // chips == span
    holds = source == span

    def res_copy():
        return remote(res_s, res_r, r_s, r_r, (sp, mate))

    @pl.when(sends_res)
    def _():
        res_s[...] = res[pl.ds(mate_row, rs), :].astype(BF16)
        res_copy().start()

    taps = gtaps.shape[1]
    last_rows = slice((chunks - 1) * cols, chunks * cols)
    blocks_here = ff // wide
    for f in range(CORES * blocks_here):
        side = f // blocks_here
        part = slice((f % blocks_here) * wide, (f % blocks_here + 1) * wide)
        here = slice(f * wide, (f + 1) * wide)
        for weight, total in ((gw, conv_g), (uw, conv_u)):
            product = total[:, here] + jnp.dot(
                rows_in[chunks - 1], weight[side, last_rows, part], preferred_element_type=F32
            )
            total[:, here] = (product * scale).astype(BF16).astype(F32)
        gate = jnp.zeros((half_rows, wide), F32)
        up = jnp.zeros((half_rows, wide), F32)
        for t in range(taps):
            begin = HALO - (taps - 1) + t
            rows = slice(begin, begin + half_rows)
            gate = gate + gtaps[side, t : t + 1, part].astype(F32) * conv_g[rows, here]
            up = up + utaps[side, t : t + 1, part].astype(F32) * conv_u[rows, here]
        hid[:, here] = (gate / (1.0 + jnp.exp(-gate)) * up).astype(BF16)

    @pl.when(holds)
    def _():
        end_r[chip] = jnp.zeros(end_r.shape[1:], BF16)

    @pl.when(jnp.logical_not(holds))
    def _():
        kept[...] = jnp.zeros(kept.shape, F32)

    shared_wait(len(shared) - 1)

    def end_copy(i, c):
        there = span * chips + i
        return remote(
            end_s.at[c, i * rs : (i + 1) * rs, :],
            end_r.at[chip, c],
            fx_s.at[i],
            fx_r.at[chip, c // (chunks - 1)],
            (sp, there),
        )

    def end_in(k, i):
        at = slice(0, chunks - 1) if i == 0 else slice(chunks - 1, chunks)
        return remote(
            end_s.at[at, 0:rs, :], end_r.at[k, at], fx_s.at[0], fx_r.at[k, i], (sp, mate)
        )

    def end_out(i):
        held = end_s.at[:, i * rs : (i + 1) * rs, :]
        return remote(held, end_r.at[chip], fx_s.at[i], fx_r.at[chip, 0], (sp, mate))

    for c in range(chunks):
        here = slice(c * cols, (c + 1) * cols)
        product = jnp.dot(hid[...], dw[:, here], preferred_element_type=F32)
        end_s[c] = product.astype(BF16)
        for i in range(chips):

            @pl.when(span * chips + i != tp)
            def _(i=i, c=c):
                end_copy(i, c).start()

            @pl.when(span * chips + i == tp)
            def _(i=i, here=here, product=product):
                kept[:, here] = product[i * rs : (i + 1) * rs, :]

    @pl.when(holds)
    def _():
        kept[...] = kept[...] + res[pl.ds(held_row, rs), :]

    @pl.when(jnp.logical_not(holds))
    def _():
        res_copy().wait_recv()
        kept[...] = res_r[...].astype(F32)

    squares = jnp.zeros((rs, 1), F32)
    sums = []
    for c in range(chunks):
        here = slice(c * cols, (c + 1) * cols)
        if c in (0, chunks - 1):
            for k in range(chips):

                @pl.when(k * CORES + (source + k) % CORES != tp)
                def _(k=k, c=c):
                    end_in(k, c // (chunks - 1)).wait_recv()

        total = kept[:, here]
        for k in range(chips):
            total = total + end_r[k, c].astype(F32)
        squares = squares + jnp.sum(total * total, axis=-1, keepdims=True)
        sums.append(total)
    scale = lax.rsqrt(squares / width + EPS)
    for c in range(chunks):
        here = slice(c * cols, (c + 1) * cols)
        out_ref[:, here] = (sums[c] * scale * fgain[:, here]).astype(BF16)

    def sent(rows, sem):
        held = kv.at[0:rows, :]
        remote(held, held, sem, d2_r.at[0], (sp, mate)).wait_send()

    if chips > 1:
        sent((chips - 1) * r, kx_s)
    q_copy(core).wait_send()
    for i in range(len(shared)):
        pushed(i, core).wait_send()
    for k in range(1, chips):
        wide_all(k, slice(0, half_rows), chunks).wait_send()
    for i in range(chips):

        @pl.when(span * chips + i != tp)
        def _(i=i):
            end_out(i).wait_send()

    @pl.when(sends_halo)
    def _():
        halo.wait_send()

    @pl.when(sends_res)
    def _():
        res_copy().wait_send()

    ring_rows = full * CORES * runs * run
    mirror_rows = ring_rows + runs * run
    for side in range(CORES if last else 1):
        extra = (len(ends) + side * len(more)) * run if last else 0

        @pl.when(jnp.logical_or(core == side, not last))
        def _(extra=extra):
            sent(mirror_rows + extra, d2_s)
            if ring_rows + extra:
                sent(ring_rows + extra, ring_s)


def solution(mesh):
    n = mesh.shape["sp"]
    chips = mesh.shape["tp"] // CORES
    head = 256

    def shards(*args):
        args = [a[None, :] if a.ndim == 1 else a for a in args]
        (target, source, _, _, qw, kw, _, ow, _, gw, _, _, _, dw, _) = args
        tgt_rows, width = target.shape
        r = source.shape[0]
        kv_heads = kw.shape[1] // head
        heads_here = qw.shape[1] // head
        rs = tgt_rows // (CORES * chips)
        half = chips * rs
        cols = width // 4
        chunks = width // cols
        ff = gw.shape[1]
        wide = 256 if ff % 256 == 0 else 128
        q_rows = heads_here * tgt_rows
        sub = max(r // RUN, 1)
        runs = chips * sub
        dma = pltpu.SemaphoreType.DMA
        shapes = [a.shape for a in args]
        for i in (9, 10, 11, 12):
            shapes[i] = (CORES,) + shapes[i]
        for i in (7, 13):
            shapes[i] = (CORES * shapes[i][0], shapes[i][1])
        scratch = [pltpu.VMEM(shape, a.dtype) for shape, a in zip(shapes, args, strict=True)]
        scratch += [
            pltpu.VMEM((kv_heads, r, 2 * head), BF16),
            pltpu.VMEM((n * CORES * chips * r, 2 * head), BF16),
            pltpu.VMEM((q_rows, head), BF16),
            pltpu.VMEM((q_rows, 1), F32),
            pltpu.VMEM((q_rows, 1), F32),
            pltpu.VMEM((q_rows, head), F32),
            pltpu.VMEM((half, CORES * heads_here * head), BF16),
            pltpu.VMEM((chunks, half, cols), BF16),
            pltpu.VMEM((max(chips - 1, 1), chunks, half, cols), BF16),
            pltpu.VMEM((CORES, heads_here * half, head), BF16),
            pltpu.VMEM((half, width), F32),
            pltpu.VMEM((chunks, HALO + half, cols), BF16),
            pltpu.VMEM((chunks, HALO, cols), BF16),
            pltpu.VMEM((HALO + half, CORES * ff), F32),
            pltpu.VMEM((HALO + half, CORES * ff), F32),
            pltpu.VMEM((half, CORES * ff), BF16),
            pltpu.VMEM((chunks, half, cols), BF16),
            pltpu.VMEM((chips, chunks, rs, cols), BF16),
            pltpu.VMEM((rs, width), F32),
            pltpu.VMEM((rs, width), BF16),
            pltpu.VMEM((rs, width), BF16),
            dma((len(args) + 2 * kv_heads,)),
            dma,
            dma((max(runs - sub, 1),)),
            dma,
            dma((max(n // 2, 1), CORES, runs)),
            dma,
            dma((max(n // 2, 1),)),
            dma((runs,)),
        ]
        scratch += [dma] * 2
        scratch += [dma((6,))] * 2
        scratch += [dma((chips,)), dma((chips, chunks + 1))]
        scratch += [dma] * 4
        scratch += [dma((chips,)), dma((chips, 2))]
        return pl.pallas_call(
            functools.partial(layer, (n, chips, kv_heads, head, heads_here, cols, sub, wide)),
            out_shape=pltpu.VMEM((rs, width), BF16),
            in_specs=[pl.BlockSpec(memory_space=pl.ANY)] * len(args),
            out_specs=pl.BlockSpec(memory_space=pltpu.VMEM),
            scratch_shapes=scratch,
            compiler_params=pltpu.CompilerParams(
                collective_id=0, has_side_effects=True, vmem_limit_bytes=60 * 1024 * 1024
            ),
        )(*args)

    in_specs = (
        P("sp", None),
        P(("sp", "tp"), None),
        P(),
        P(),
        P(None, "tp"),
        P(),
        P(),
        P("tp", None),
        P(),
        P(None, "tp"),
        P(None, "tp"),
        P(None, "tp"),
        P(None, "tp"),
        P("tp", None),
        P(),
    )
    return jax.shard_map(
        shards, mesh=mesh, in_specs=in_specs, out_specs=P(("sp", "tp"), None), check_vma=False
    )
```

```python
import functools

import jax
import jax.numpy as jnp
from jax import lax
from jax.experimental import pallas as pl
from jax.experimental.pallas import tpu as pltpu
from jax.sharding import PartitionSpec as P

MESH = pl.DeviceIdType.MESH
EPS = 1e-06
HALO = 16
RUN = 32
CORES = 2
SPLIT = 8
F32 = jnp.float32
BF16 = jnp.bfloat16


def normed(values, gain):
    wide = values.astype(F32)
    scale = lax.rsqrt(jnp.mean(wide * wide, axis=-1, keepdims=True) + EPS)
    return (wide * scale * gain).astype(BF16)


def layer(
    dims,
    target_h,
    source_h,
    qgain_h,
    sgain_h,
    qw_h,
    kw_h,
    vw_h,
    ow_h,
    mgain_h,
    gw_h,
    uw_h,
    gtaps_h,
    utaps_h,
    dw_h,
    fgain_h,
    out_ref,
    tgt,
    src,
    qgain,
    sgain,
    qw,
    kw,
    vw,
    ow,
    mgain,
    gw,
    uw,
    gtaps,
    utaps,
    dw,
    fgain,
    kvh,
    kv,
    q2,
    top,
    tot,
    acc,
    att,
    chip_s,
    chip_r,
    q_held,
    res,
    rows_in,
    halo_s,
    conv_g,
    conv_u,
    hid,
    end_s,
    end_r,
    kept,
    res_s,
    res_r,
    load_sem,
    kx_s,
    kx_r,
    ring_s,
    ring_r,
    d2_s,
    d2_r,
    d2_first,
    q_s,
    q_r,
    w_s,
    w_r,
    bx_s,
    bx_r,
    h_s,
    h_r,
    r_s,
    r_r,
    fx_s,
    fx_r,
):
    n, chips, kv_heads, head, heads_here, cols, sub, wide = dims
    tgt_rows, width = tgt.shape
    r = src.shape[0]
    rs = tgt_rows // (CORES * chips)
    half_rows = chips * rs
    run = r // sub
    runs = chips * sub
    chunks = width // cols
    ff = gw_h.shape[1]
    sp = lax.axis_index("sp")
    tp = lax.axis_index("tp")
    chip = tp // CORES
    core = tp % CORES
    mate = tp + 1 - 2 * core
    span = (core + chip) % CORES
    base = pl.multiple_of(span * half_rows, half_rows)

    def chip_at(k):
        return (chip + k) % chips

    def ring_at(p):
        if n % 2:
            return p
        upper = p // (n // 2)
        return 2 * (p * (1 - upper) + (n - 1 - p) * upper) + upper

    if n % 2:
        pos = sp
    else:
        pos = (sp // 2) * (1 - sp % 2) + (n - 1 - sp // 2) * (sp % 2)
    ahead = ring_at((pos + 1) % n)
    behind = ring_at((pos + n - 1) % n)

    def load(index, hbm, vmem):
        copy = pltpu.make_async_copy(hbm, vmem, load_sem.at[index])
        copy.start()
        return copy

    def head_of(c):
        return (c * CORES * kv_heads) // (chips * CORES)

    own_head = head_of(chip)
    order = [(own_head + 1 + g) % kv_heads for g in range(kv_heads)]

    def columns(g):
        return pl.ds(pl.multiple_of(g * head, head), head)

    first = [load(0, source_h, src), load(1, sgain_h, sgain)]
    by_head = [
        [
            load(2 + 2 * i, kw_h.at[:, columns(g)], kw.at[:, columns(g)]),
            load(3 + 2 * i, vw_h.at[:, columns(g)], vw.at[:, columns(g)]),
        ]
        for i, g in enumerate(order)
    ]
    used = 2 + 2 * kv_heads

    barrier = pltpu.get_barrier_semaphore()
    following = (sp + 1) % n
    peers = [(ahead, tp), (behind, tp), (sp, mate)]
    peers += [(sp, chip_at(k) * CORES + i) for k in range(1, chips) for i in range(CORES)]
    for peer in peers:
        pl.semaphore_signal(barrier, inc=1, device_id=peer, device_id_type=MESH)

    def remote(source_ref, dest_ref, send, recv, device):
        return pltpu.make_async_remote_copy(
            src_ref=source_ref,
            dst_ref=dest_ref,
            send_sem=send,
            recv_sem=recv,
            device_id=device,
            device_id_type=MESH,
        )

    def block(slot, lineage, j):
        start = ((slot * CORES + lineage) * runs + j) * run
        if not isinstance(start, int):
            start = pl.multiple_of(start, run)
        return kv.at[pl.ds(start, run), :]

    def chip_copy(j, half):
        there = chip_at(j // sub)
        at = slice(half * head, (half + 1) * head)
        return remote(
            kvh.at[head_of(there), (j % sub) * run : (j % sub + 1) * run, at],
            block(0, core, j).at[:, at],
            kx_s,
            kx_r.at[j - sub, half],
            (sp, there * CORES + core),
        )

    last = n // 2 if n % 2 == 0 else 0
    full = (n - 1) // 2
    own = range(sub)
    far = range(sub, runs)
    onward = ahead * (1 - core) + behind * core

    def slot_of(d, side):
        if isinstance(d, int) and d == 0:
            return 0
        if isinstance(d, int) and d == last:
            return n - 1
        return 2 * d - 1 + side

    def ring_copy(d, rel, j):
        lineage = core * (1 - rel) + (1 - core) * rel
        return remote(
            block(slot_of(d - 1, core), lineage, j),
            block(slot_of(d, core), lineage, j),
            ring_s,
            ring_r.at[d - 1, rel, j],
            (onward, tp),
        )

    def mirror_copy(d, rel, j, side):
        lineage = side * (1 - rel) + (1 - side) * rel
        held = block(slot_of(d, side), lineage, j)
        first = isinstance(d, int) and d == 0
        return remote(held, held, d2_s, d2_first.at[j] if first else d2_r.at[d - 1], (sp, mate))

    def mirror_out(d, rel, j):
        return mirror_copy(d, rel, j, core)

    def mirror_in(d, rel, j):
        return mirror_copy(d, rel, j, 1 - core)

    def whole(w, side):
        high = w.shape[0] // CORES
        return w.at[pl.ds(pl.multiple_of(side * high, high), high), :]

    shared = [
        (ow_h, lambda side: whole(ow, side), SPLIT),
        (gw_h, lambda side: gw.at[side], SPLIT),
        (uw_h, lambda side: uw.at[side], SPLIT),
        (gtaps_h, lambda side: gtaps.at[side], 1),
        (utaps_h, lambda side: utaps.at[side], 1),
        (dw_h, lambda side: whole(dw, side), SPLIT),
    ]

    def push(i, p, side):
        held, place, pieces = shared[i]
        high = held.shape[0] // pieces
        at = slice(p * high, (p + 1) * high)
        there = place(side)
        return remote(
            held.at[at, :], there.at[at, :], w_s.at[i], w_r.at[i], (sp, mate)
        )

    def pushed(i, side):
        held, place, _ = shared[i]
        return remote(held, place(side), w_s.at[i], w_r.at[i], (sp, mate))

    pending = [(i, p) for i in range(len(shared)) for p in range(shared[i][2])]

    def feed(count):
        for x in pending[:count]:
            push(*x, core).start()
        del pending[:count]

    def shared_wait(i):
        pushed(i, 1 - core).wait_recv()

    def launch(j):
        if full >= 1 or (last and (0, j) in ends):
            ring_copy(1, 0, j).start()
        elif last:

            @pl.when(core == 1)
            def _():
                ring_copy(1, 0, j).start()

        mirror_out(0, 0, j).start()

    def launch_mate(blocks):
        for j in blocks:
            mirror_in(0, 0, j).wait_recv()
            if full >= 1:
                ring_copy(1, 1, j).start()
            elif last and (1, j) in more:

                @pl.when(core == 1)
                def _(j=j):
                    ring_copy(1, 1, j).start()

    def launch_far():
        for j in far:
            chip_copy(j, 0).wait_recv()
            chip_copy(j, 1).wait_recv()
            launch(j)

    quota = {1: 6, 2: 5, 3: 1}
    ends = [(0, j) for j in own]
    more = [(rel, j) for rel in range(CORES) for j in far]

    def arrive(d, rel, blocks):
        end = isinstance(d, int) and d == full
        for j in blocks:
            ring_copy(d, rel, j).wait_recv()
            if not end or (last and (rel, j) in ends):
                ring_copy(d + 1, rel, j).start()
            elif last and (rel, j) in more:

                @pl.when(core == 1)
                def _(rel=rel, j=j):
                    ring_copy(last, rel, j).start()

            mirror_out(d, rel, j).start()
            if isinstance(d, int) and d in quota and quota[d] > 0:
                quota[d] -= 1
                feed(1)

    def arrive_last():
        if last:
            for rel, j in ends:
                ring_copy(last, rel, j).wait_recv()
                mirror_out(last, rel, j).start()

            if more:

                @pl.when(core == 1)
                def _():
                    for rel, j in more:
                        ring_copy(last, rel, j).wait_recv()
                        mirror_out(last, rel, j).start()

    for copy in first:
        copy.wait()
    source_in = normed(src[...], sgain[...])
    second = [
        load(used + i, a, b)
        for i, (a, b) in enumerate(((target_h, tgt), (qgain_h, qgain), (qw_h, qw)))
    ]
    early = chips == kv_heads

    def send_far(half):
        for j in far:
            chip_copy(j, half).start()

    for i, g in enumerate(order):
        for half, copy in enumerate(by_head[i]):
            if i == 0 or half == 0:
                for waited in by_head[i] if i else [copy]:
                    waited.wait()
            weight = (kw, vw)[half]
            product = jnp.dot(source_in, weight[:, columns(g)], preferred_element_type=F32)
            kvh[g, :, half * head : (half + 1) * head] = product.astype(BF16)
            if i == (kv_heads - 2 if early else kv_heads - 1):
                if half == 0:
                    pl.semaphore_wait(barrier, len(peers))
                send_far(half)
    kv[pl.ds(pl.multiple_of(core * chips * r, r), r), :] = kvh[own_head]
    for j in range(sub):
        launch(j)
    for copy in second:
        copy.wait()
    queries = jnp.dot(normed(tgt[...], qgain[...]), qw[...], preferred_element_type=F32).astype(
        BF16
    )
    group = heads_here * half_rows
    for side in range(CORES):
        for h in range(heads_here):
            q_held[side, h * half_rows : (h + 1) * half_rows, :] = queries[
                side * half_rows : (side + 1) * half_rows, h * head : (h + 1) * head
            ]

    def q_copy(side):
        return remote(
            q_held.at[1 - span],
            q2.at[pl.ds(pl.multiple_of(side * group, group), group), :],
            q_s,
            q_r,
            (sp, mate),
        )

    q_copy(core).start()
    q2[pl.ds(pl.multiple_of(core * group, group), group), :] = q_held[span]
    top[...] = jnp.full(top.shape, -1e30, F32)
    tot[...] = jnp.zeros(tot.shape, F32)
    acc[...] = jnp.zeros(acc.shape, F32)

    slot_rows = CORES * chips * r

    def attend(slot, slots):
        start = slot * slot_rows
        if not isinstance(start, int):
            start = pl.multiple_of(start, slot_rows)
        here = pl.ds(start, slots * slot_rows)
        scores = lax.dot_general(
            q2[...], kv[here, :head], (((1,), (1,)), ((), ())), preferred_element_type=F32
        ) * (head**-0.5)
        old = top[...]
        new = jnp.maximum(old, jnp.max(scores, axis=-1, keepdims=True))
        shrink = jnp.exp(old - new)
        probs = jnp.exp(scores - new)
        top[...] = new
        tot[...] = tot[...] * shrink + jnp.sum(probs, axis=-1, keepdims=True)
        acc[...] = acc[...] * shrink + jnp.dot(
            probs.astype(BF16), kv[here, head:], preferred_element_type=F32
        )

    def local_loads():
        pairs = [(held, place(core)) for held, place, _ in shared]
        pairs += [(mgain_h, mgain), (fgain_h, fgain)]
        return [load(used + 3 + i, a, b) for i, (a, b) in enumerate(pairs)]

    def mirror_wait(d, start, rows):
        held = kv.at[pl.ds(start, rows), :]
        remote(held, held, d2_s, d2_r.at[d - 1], (sp, mate)).wait_recv()

    def mirrored(d):
        if isinstance(d, int) and d == last:
            begin = (n - 1) * slot_rows

            @pl.when(core == 1)
            def _():
                mirror_wait(d, begin, len(ends) * run)

            if more:

                @pl.when(core == 0)
                def _():
                    mirror_wait(d, begin + len(ends) * run, slot_rows - len(ends) * run)
        else:
            start = slot_of(d, 1 - core) * slot_rows
            mirror_wait(d, pl.multiple_of(start, slot_rows), slot_rows)

    def wave(d):
        for blocks in (own, far):
            for rel in range(CORES):
                arrive(d, rel, blocks)

    if full >= 1:
        feed(4)
        launch_mate(own)
        launch_far()
        feed(3)
        launch_mate(far)
        q_copy(1 - core).wait_recv()
        wave(1)
        rest = local_loads()
        done = 1
        if full > 4:
            wave(2)
            attend(0, 1)

            def middle(d, carry):
                wave(d)
                mirrored(d - 2)
                attend(2 * d - 5, 2)
                return carry

            lax.fori_loop(3, full, middle, 0)
            wave(full)
            done = full - 2
        else:
            for d in range(2, full + 1):
                wave(d)
        start = 2 * done - 1 if full > 4 else 0
        for d in range(done, full):
            mirrored(d)
        attend(start, 2 * full - 1 - start)
        arrive_last()
        feed(len(pending) - SPLIT // 2)
        mirrored(full)
        attend(2 * full - 1, 2)
    else:
        rest = local_loads()
        launch_far()
        launch_mate(range(runs))
        q_copy(1 - core).wait_recv()
        arrive_last()
        feed(3 * SPLIT + 2)
        attend(0, 1)
    if last:
        mirrored(last)
        attend(n - 1, 1)

    attended = (acc[...] / tot[...]).astype(BF16)
    for h in range(CORES * heads_here):
        att[:, h * head : (h + 1) * head] = attended[h * half_rows : (h + 1) * half_rows, :]
    for copy in rest:
        copy.wait()
    shared_wait(0)

    body_rows = half_rows - HALO
    body = slice(0, body_rows)
    tail = slice(body_rows, half_rows)

    def peer_of(k):
        there = chip_at(k)
        return there * CORES + (span + there) % CORES

    def wide_copy(k, c, i):
        at = (body, tail)[i]
        return remote(
            chip_s.at[c, at, :],
            chip_r.at[k - 1, c, at, :],
            bx_s.at[k],
            bx_r.at[k, c * (1 - i) + chunks * i],
            (sp, peer_of(k)),
        )

    for c in range(chunks):
        here = slice(c * cols, (c + 1) * cols)
        product = jnp.dot(att[...], ow[:, here], preferred_element_type=F32)
        chip_s[c] = product.astype(BF16)
        for k in range(1, chips):
            wide_copy(k, c, 1).start()
        res[:, here] = product + tgt[pl.ds(base, half_rows), here].astype(F32)
    for c in range(chunks):
        for k in range(1, chips):
            wide_copy(k, c, 0).start()

    def wide_all(k, at, recv):
        return remote(
            chip_s.at[:, at, :],
            chip_r.at[k - 1, :, at, :],
            bx_s.at[k],
            bx_r.at[k, recv],
            (sp, peer_of(k)),
        )

    def settle(c, i):
        at = (body, tail)[i]
        here = slice(c * cols, (c + 1) * cols)
        residual = res[at, here]
        for k in range(1, chips):
            if i == 0:
                wide_copy(k, c, 0).wait_recv()
            residual = residual + chip_r[k - 1, c, at, :].astype(F32)
        residual = residual.astype(BF16).astype(F32)
        res[at, here] = residual
        return jnp.sum(residual * residual, axis=-1, keepdims=True)

    for k in range(1, chips):
        wide_all(k, tail, chunks).wait_recv()

    beyond = sp * (1 - span) + following * span

    halo = remote(halo_s, rows_in.at[:, 0:HALO, :], h_s, h_r.at[0], (beyond, mate))

    def halo_copy(c):
        return remote(
            halo_s.at[c], rows_in.at[c, 0:HALO, :], h_s, h_r.at[c], (beyond, mate)
        )

    sends_halo = jnp.logical_or(span == 0, sp < n - 1)
    takes_halo = jnp.logical_or(span == 1, sp > 0)
    tail_squares = settle(0, 1)
    for c in range(1, chunks):
        tail_squares = tail_squares + settle(c, 1)
    scale = lax.rsqrt(tail_squares / width + EPS)
    for c in range(chunks):
        here = slice(c * cols, (c + 1) * cols)
        halo_s[c] = (res[tail, here] * scale * mgain[:, here]).astype(BF16)

    @pl.when(sends_halo)
    def _():
        for c in range(chunks):
            halo_copy(c).start()

    feed(len(pending))

    @pl.when(jnp.logical_not(takes_halo))
    def _():
        rows_in[:, 0:HALO, :] = jnp.zeros((chunks, HALO, cols), BF16)

    def ready(c):
        @pl.when(takes_halo)
        def _():
            halo_copy(c).wait_recv()

    def mix(c):
        here = slice(c * cols, (c + 1) * cols)
        for side in range(CORES):
            there = slice(side * ff, (side + 1) * ff)
            for weight, total in ((gw, conv_g), (uw, conv_u)):
                product = jnp.dot(
                    rows_in[c], weight[side, here, :], preferred_element_type=F32
                )
                if c > 0:
                    product = product + total[:, there]
                total[:, there] = product

    for i in range(1, len(shared) - 1):
        shared_wait(i)
    squares = jnp.zeros((body_rows, 1), F32)
    for c in range(chunks):
        squares = squares + settle(c, 0)
        here = slice(c * cols, (c + 1) * cols)
        rows_in[c, HALO:, :] = (res[:, here] * mgain[:, here]).astype(BF16)
        if 0 < c < chunks - 1:
            for i in range(0 if c == 1 else c, c + 1):
                ready(i)
                mix(i)
    ready(chunks - 1)
    squares = jnp.concatenate([squares, tail_squares], axis=0)
    scale = jnp.concatenate(
        [jnp.ones((HALO, 1), F32), lax.rsqrt(squares / width + EPS)], axis=0
    )

    source = tp // chips
    held_row = pl.multiple_of((tp % chips) * rs, rs)
    mate_row = pl.multiple_of((mate % chips) * rs, rs)
    sends_res = mate // chips == span
    holds = source == span

    def res_copy():
        return remote(res_s, res_r, r_s, r_r, (sp, mate))

    @pl.when(sends_res)
    def _():
        res_s[...] = res[pl.ds(mate_row, rs), :].astype(BF16)
        res_copy().start()

    taps = gtaps.shape[1]
    last_rows = slice((chunks - 1) * cols, chunks * cols)
    blocks_here = ff // wide
    for f in range(CORES * blocks_here):
        side = f // blocks_here
        part = slice((f % blocks_here) * wide, (f % blocks_here + 1) * wide)
        here = slice(f * wide, (f + 1) * wide)
        for weight, total in ((gw, conv_g), (uw, conv_u)):
            product = total[:, here] + jnp.dot(
                rows_in[chunks - 1], weight[side, last_rows, part], preferred_element_type=F32
            )
            total[:, here] = (product * scale).astype(BF16).astype(F32)
        gate = jnp.zeros((half_rows, wide), F32)
        up = jnp.zeros((half_rows, wide), F32)
        for t in range(taps):
            begin = HALO - (taps - 1) + t
            rows = slice(begin, begin + half_rows)
            gate = gate + gtaps[side, t : t + 1, part].astype(F32) * conv_g[rows, here]
            up = up + utaps[side, t : t + 1, part].astype(F32) * conv_u[rows, here]
        hid[:, here] = (gate / (1.0 + jnp.exp(-gate)) * up).astype(BF16)

    @pl.when(holds)
    def _():
        end_r[chip] = jnp.zeros(end_r.shape[1:], BF16)

    @pl.when(jnp.logical_not(holds))
    def _():
        kept[...] = jnp.zeros(kept.shape, F32)

    shared_wait(len(shared) - 1)

    def end_copy(i, c):
        there = span * chips + i
        return remote(
            end_s.at[c, i * rs : (i + 1) * rs, :],
            end_r.at[chip, c],
            fx_s.at[i],
            fx_r.at[chip, c // (chunks - 1)],
            (sp, there),
        )

    def end_in(k, i):
        at = slice(0, chunks - 1) if i == 0 else slice(chunks - 1, chunks)
        return remote(
            end_s.at[at, 0:rs, :], end_r.at[k, at], fx_s.at[0], fx_r.at[k, i], (sp, mate)
        )

    def end_out(i):
        held = end_s.at[:, i * rs : (i + 1) * rs, :]
        return remote(held, end_r.at[chip], fx_s.at[i], fx_r.at[chip, 0], (sp, mate))

    for c in range(chunks):
        here = slice(c * cols, (c + 1) * cols)
        product = jnp.dot(hid[...], dw[:, here], preferred_element_type=F32)
        end_s[c] = product.astype(BF16)
        for i in range(chips):

            @pl.when(span * chips + i != tp)
            def _(i=i, c=c):
                end_copy(i, c).start()

            @pl.when(span * chips + i == tp)
            def _(i=i, here=here, product=product):
                kept[:, here] = product[i * rs : (i + 1) * rs, :]

    @pl.when(holds)
    def _():
        kept[...] = kept[...] + res[pl.ds(held_row, rs), :]

    @pl.when(jnp.logical_not(holds))
    def _():
        res_copy().wait_recv()
        kept[...] = res_r[...].astype(F32)

    squares = jnp.zeros((rs, 1), F32)
    sums = []
    for c in range(chunks):
        here = slice(c * cols, (c + 1) * cols)
        if c in (0, chunks - 1):
            for k in range(chips):

                @pl.when(k * CORES + (source + k) % CORES != tp)
                def _(k=k, c=c):
                    end_in(k, c // (chunks - 1)).wait_recv()

        total = kept[:, here]
        for k in range(chips):
            total = total + end_r[k, c].astype(F32)
        squares = squares + jnp.sum(total * total, axis=-1, keepdims=True)
        sums.append(total)
    scale = lax.rsqrt(squares / width + EPS)
    for c in range(chunks):
        here = slice(c * cols, (c + 1) * cols)
        out_ref[:, here] = (sums[c] * scale * fgain[:, here]).astype(BF16)

    def sent(rows, sem):
        held = kv.at[0:rows, :]
        remote(held, held, sem, d2_r.at[0], (sp, mate)).wait_send()

    if chips > 1:
        sent((chips - 1) * r, kx_s)
    q_copy(core).wait_send()
    for i in range(len(shared)):
        pushed(i, core).wait_send()
    for k in range(1, chips):
        wide_all(k, slice(0, half_rows), chunks).wait_send()
    for i in range(chips):

        @pl.when(span * chips + i != tp)
        def _(i=i):
            end_out(i).wait_send()

    @pl.when(sends_halo)
    def _():
        halo.wait_send()

    @pl.when(sends_res)
    def _():
        res_copy().wait_send()

    ring_rows = full * CORES * runs * run
    mirror_rows = ring_rows + runs * run
    for side in range(CORES if last else 1):
        extra = (len(ends) + side * len(more)) * run if last else 0

        @pl.when(jnp.logical_or(core == side, not last))
        def _(extra=extra):
            sent(mirror_rows + extra, d2_s)
            if ring_rows + extra:
                sent(ring_rows + extra, ring_s)


def solution(mesh):
    n = mesh.shape["sp"]
    chips = mesh.shape["tp"] // CORES
    head = 256

    def shards(*args):
        args = [a[None, :] if a.ndim == 1 else a for a in args]
        (target, source, _, _, qw, kw, _, ow, _, gw, _, _, _, dw, _) = args
        tgt_rows, width = target.shape
        r = source.shape[0]
        kv_heads = kw.shape[1] // head
        heads_here = qw.shape[1] // head
        rs = tgt_rows // (CORES * chips)
        half = chips * rs
        cols = width // 4
        chunks = width // cols
        ff = gw.shape[1]
        wide = 256 if ff % 256 == 0 else 128
        q_rows = heads_here * tgt_rows
        sub = max(r // RUN, 1)
        runs = chips * sub
        dma = pltpu.SemaphoreType.DMA
        shapes = [a.shape for a in args]
        for i in (9, 10, 11, 12):
            shapes[i] = (CORES,) + shapes[i]
        for i in (7, 13):
            shapes[i] = (CORES * shapes[i][0], shapes[i][1])
        scratch = [pltpu.VMEM(shape, a.dtype) for shape, a in zip(shapes, args, strict=True)]
        scratch += [
            pltpu.VMEM((kv_heads, r, 2 * head), BF16),
            pltpu.VMEM((n * CORES * chips * r, 2 * head), BF16),
            pltpu.VMEM((q_rows, head), BF16),
            pltpu.VMEM((q_rows, 1), F32),
            pltpu.VMEM((q_rows, 1), F32),
            pltpu.VMEM((q_rows, head), F32),
            pltpu.VMEM((half, CORES * heads_here * head), BF16),
            pltpu.VMEM((chunks, half, cols), BF16),
            pltpu.VMEM((max(chips - 1, 1), chunks, half, cols), BF16),
            pltpu.VMEM((CORES, heads_here * half, head), BF16),
            pltpu.VMEM((half, width), F32),
            pltpu.VMEM((chunks, HALO + half, cols), BF16),
            pltpu.VMEM((chunks, HALO, cols), BF16),
            pltpu.VMEM((HALO + half, CORES * ff), F32),
            pltpu.VMEM((HALO + half, CORES * ff), F32),
            pltpu.VMEM((half, CORES * ff), BF16),
            pltpu.VMEM((chunks, half, cols), BF16),
            pltpu.VMEM((chips, chunks, rs, cols), BF16),
            pltpu.VMEM((rs, width), F32),
            pltpu.VMEM((rs, width), BF16),
            pltpu.VMEM((rs, width), BF16),
            dma((len(args) + 2 * kv_heads,)),
            dma,
            dma((max(runs - sub, 1), 2)),
            dma,
            dma((max(n // 2, 1), CORES, runs)),
            dma,
            dma((max(n // 2, 1),)),
            dma((runs,)),
        ]
        scratch += [dma] * 2
        scratch += [dma((6,))] * 2
        scratch += [dma((chips,)), dma((chips, chunks + 1))]
        scratch += [dma, dma((chunks,)), dma, dma]
        scratch += [dma((chips,)), dma((chips, 2))]
        return pl.pallas_call(
            functools.partial(layer, (n, chips, kv_heads, head, heads_here, cols, sub, wide)),
            out_shape=pltpu.VMEM((rs, width), BF16),
            in_specs=[pl.BlockSpec(memory_space=pl.ANY)] * len(args),
            out_specs=pl.BlockSpec(memory_space=pltpu.VMEM),
            scratch_shapes=scratch,
            compiler_params=pltpu.CompilerParams(
                collective_id=0, has_side_effects=True, vmem_limit_bytes=60 * 1024 * 1024
            ),
        )(*args)

    in_specs = (
        P("sp", None),
        P(("sp", "tp"), None),
        P(),
        P(),
        P(None, "tp"),
        P(),
        P(),
        P("tp", None),
        P(),
        P(None, "tp"),
        P(None, "tp"),
        P(None, "tp"),
        P(None, "tp"),
        P("tp", None),
        P(),
    )
    return jax.shard_map(
        shards, mesh=mesh, in_specs=in_specs, out_specs=P(("sp", "tp"), None), check_vma=False
    )
```

```python
import functools

import jax
import jax.numpy as jnp
from jax import lax
from jax.experimental import pallas as pl
from jax.experimental.pallas import tpu as pltpu
from jax.sharding import PartitionSpec as P

MESH = pl.DeviceIdType.MESH
EPS = 1e-06
HALO = 16
RUN = 32
CORES = 2
SPLIT = 8
F32 = jnp.float32
BF16 = jnp.bfloat16


def normed(values, gain):
    wide = values.astype(F32)
    scale = lax.rsqrt(jnp.mean(wide * wide, axis=-1, keepdims=True) + EPS)
    return (wide * scale * gain).astype(BF16)


def layer(
    dims,
    target_h,
    source_h,
    qgain_h,
    sgain_h,
    qw_h,
    kw_h,
    vw_h,
    ow_h,
    mgain_h,
    gw_h,
    uw_h,
    gtaps_h,
    utaps_h,
    dw_h,
    fgain_h,
    out_ref,
    tgt,
    src,
    qgain,
    sgain,
    qw,
    kw,
    vw,
    ow,
    mgain,
    gw,
    uw,
    gtaps,
    utaps,
    dw,
    fgain,
    kvh,
    kv,
    q2,
    top,
    tot,
    acc,
    att,
    chip_s,
    chip_r,
    q_held,
    res,
    rows_in,
    halo_s,
    conv_g,
    conv_u,
    hid,
    end_s,
    end_r,
    kept,
    res_s,
    res_r,
    load_sem,
    kx_s,
    kx_r,
    ring_s,
    ring_r,
    d2_s,
    d2_r,
    d2_first,
    q_s,
    q_r,
    w_s,
    w_r,
    bx_s,
    bx_r,
    h_s,
    h_r,
    r_s,
    r_r,
    fx_s,
    fx_r,
):
    n, chips, kv_heads, head, heads_here, cols, sub, wide = dims
    tgt_rows, width = tgt.shape
    r = src.shape[0]
    rs = tgt_rows // (CORES * chips)
    half_rows = chips * rs
    run = r // sub
    runs = chips * sub
    chunks = width // cols
    ff = gw_h.shape[1]
    sp = lax.axis_index("sp")
    tp = lax.axis_index("tp")
    chip = tp // CORES
    core = tp % CORES
    mate = tp + 1 - 2 * core
    span = (core + chip) % CORES
    base = pl.multiple_of(span * half_rows, half_rows)

    def chip_at(k):
        return (chip + k) % chips

    def ring_at(p):
        if n % 2:
            return p
        upper = p // (n // 2)
        return 2 * (p * (1 - upper) + (n - 1 - p) * upper) + upper

    if n % 2:
        pos = sp
    else:
        pos = (sp // 2) * (1 - sp % 2) + (n - 1 - sp // 2) * (sp % 2)
    ahead = ring_at((pos + 1) % n)
    behind = ring_at((pos + n - 1) % n)

    def load(index, hbm, vmem):
        copy = pltpu.make_async_copy(hbm, vmem, load_sem.at[index])
        copy.start()
        return copy

    def head_of(c):
        return (c * CORES * kv_heads) // (chips * CORES)

    own_head = head_of(chip)
    order = [(own_head + 1 + g) % kv_heads for g in range(kv_heads)]

    def columns(g):
        return pl.ds(pl.multiple_of(g * head, head), head)

    first = [load(0, source_h, src), load(1, sgain_h, sgain)]
    by_head = [
        [
            load(2 + 2 * i, kw_h.at[:, columns(g)], kw.at[:, columns(g)]),
            load(3 + 2 * i, vw_h.at[:, columns(g)], vw.at[:, columns(g)]),
        ]
        for i, g in enumerate(order)
    ]
    used = 2 + 2 * kv_heads

    barrier = pltpu.get_barrier_semaphore()
    following = (sp + 1) % n
    peers = [(ahead, tp), (behind, tp), (sp, mate)]
    peers += [(sp, chip_at(k) * CORES + i) for k in range(1, chips) for i in range(CORES)]
    for peer in peers:
        pl.semaphore_signal(barrier, inc=1, device_id=peer, device_id_type=MESH)

    def remote(source_ref, dest_ref, send, recv, device):
        return pltpu.make_async_remote_copy(
            src_ref=source_ref,
            dst_ref=dest_ref,
            send_sem=send,
            recv_sem=recv,
            device_id=device,
            device_id_type=MESH,
        )

    def block(slot, lineage, j):
        start = ((slot * CORES + lineage) * runs + j) * run
        if not isinstance(start, int):
            start = pl.multiple_of(start, run)
        return kv.at[pl.ds(start, run), :]

    def chip_copy(j, half):
        there = chip_at(j // sub)
        at = slice(half * head, (half + 1) * head)
        return remote(
            kvh.at[head_of(there), (j % sub) * run : (j % sub + 1) * run, at],
            block(0, core, j).at[:, at],
            kx_s,
            kx_r.at[j - sub, half],
            (sp, there * CORES + core),
        )

    last = n // 2 if n % 2 == 0 else 0
    full = (n - 1) // 2
    own = range(sub)
    far = range(sub, runs)
    onward = ahead * (1 - core) + behind * core

    def slot_of(d, side):
        if isinstance(d, int) and d == 0:
            return 0
        if isinstance(d, int) and d == last:
            return n - 1
        return 2 * d - 1 + side

    def ring_copy(d, rel, j):
        lineage = core * (1 - rel) + (1 - core) * rel
        return remote(
            block(slot_of(d - 1, core), lineage, j),
            block(slot_of(d, core), lineage, j),
            ring_s,
            ring_r.at[d - 1, rel, j],
            (onward, tp),
        )

    def mirror_copy(d, rel, j, side):
        lineage = side * (1 - rel) + (1 - side) * rel
        held = block(slot_of(d, side), lineage, j)
        first = isinstance(d, int) and d == 0
        return remote(held, held, d2_s, d2_first.at[j] if first else d2_r.at[d - 1], (sp, mate))

    def mirror_out(d, rel, j):
        return mirror_copy(d, rel, j, core)

    def mirror_in(d, rel, j):
        return mirror_copy(d, rel, j, 1 - core)

    def whole(w, side):
        high = w.shape[0] // CORES
        return w.at[pl.ds(pl.multiple_of(side * high, high), high), :]

    shared = [
        (ow_h, lambda side: whole(ow, side), SPLIT),
        (gw_h, lambda side: gw.at[side], SPLIT),
        (uw_h, lambda side: uw.at[side], SPLIT),
        (gtaps_h, lambda side: gtaps.at[side], 1),
        (utaps_h, lambda side: utaps.at[side], 1),
        (dw_h, lambda side: whole(dw, side), SPLIT),
    ]

    def push(i, p, side):
        held, place, pieces = shared[i]
        high = held.shape[0] // pieces
        at = slice(p * high, (p + 1) * high)
        there = place(side)
        return remote(
            held.at[at, :], there.at[at, :], w_s.at[i], w_r.at[i], (sp, mate)
        )

    def pushed(i, side):
        held, place, _ = shared[i]
        return remote(held, place(side), w_s.at[i], w_r.at[i], (sp, mate))

    pending = [(i, p) for i in range(len(shared)) for p in range(shared[i][2])]

    def feed(count):
        for x in pending[:count]:
            push(*x, core).start()
        del pending[:count]

    def shared_wait(i):
        pushed(i, 1 - core).wait_recv()

    def launch(j):
        if full >= 1 or (last and (0, j) in ends):
            ring_copy(1, 0, j).start()
        elif last:

            @pl.when(core == 1)
            def _():
                ring_copy(1, 0, j).start()

        mirror_out(0, 0, j).start()

    def launch_mate(blocks):
        for j in blocks:
            mirror_in(0, 0, j).wait_recv()
            if full >= 1:
                ring_copy(1, 1, j).start()
            elif last and (1, j) in more:

                @pl.when(core == 1)
                def _(j=j):
                    ring_copy(1, 1, j).start()

    def launch_far():
        for j in far:
            chip_copy(j, 0).wait_recv()
            chip_copy(j, 1).wait_recv()
            launch(j)

    quota = {1: 6, 2: 5, 3: 1}
    ends = [(0, j) for j in own]
    more = [(rel, j) for rel in range(CORES) for j in far]

    def arrive(d, rel, blocks):
        end = isinstance(d, int) and d == full
        for j in blocks:
            ring_copy(d, rel, j).wait_recv()
            if not end or (last and (rel, j) in ends):
                ring_copy(d + 1, rel, j).start()
            elif last and (rel, j) in more:

                @pl.when(core == 1)
                def _(rel=rel, j=j):
                    ring_copy(last, rel, j).start()

            mirror_out(d, rel, j).start()
            if isinstance(d, int) and d in quota and quota[d] > 0:
                quota[d] -= 1
                feed(1)

    def arrive_last():
        if last:
            for rel, j in ends:
                ring_copy(last, rel, j).wait_recv()
                mirror_out(last, rel, j).start()

            if more:

                @pl.when(core == 1)
                def _():
                    for rel, j in more:
                        ring_copy(last, rel, j).wait_recv()
                        mirror_out(last, rel, j).start()

    for copy in first:
        copy.wait()
    source_in = normed(src[...], sgain[...])
    second = [
        load(used + i, a, b)
        for i, (a, b) in enumerate(((target_h, tgt), (qgain_h, qgain), (qw_h, qw)))
    ]
    early = chips == kv_heads

    def send_far(half):
        for j in far:
            chip_copy(j, half).start()

    for i, g in enumerate(order):
        for half, copy in enumerate(by_head[i]):
            if i == 0 or half == 0:
                for waited in by_head[i] if i else [copy]:
                    waited.wait()
            weight = (kw, vw)[half]
            product = jnp.dot(source_in, weight[:, columns(g)], preferred_element_type=F32)
            kvh[g, :, half * head : (half + 1) * head] = product.astype(BF16)
            if i == (kv_heads - 2 if early else kv_heads - 1):
                if half == 0:
                    pl.semaphore_wait(barrier, len(peers))
                send_far(half)
    kv[pl.ds(pl.multiple_of(core * chips * r, r), r), :] = kvh[own_head]
    for j in range(sub):
        launch(j)
    for copy in second:
        copy.wait()
    queries = jnp.dot(normed(tgt[...], qgain[...]), qw[...], preferred_element_type=F32).astype(
        BF16
    )
    group = heads_here * half_rows
    for side in range(CORES):
        for h in range(heads_here):
            q_held[side, h * half_rows : (h + 1) * half_rows, :] = queries[
                side * half_rows : (side + 1) * half_rows, h * head : (h + 1) * head
            ]

    def q_copy(side):
        return remote(
            q_held.at[1 - span],
            q2.at[pl.ds(pl.multiple_of(side * group, group), group), :],
            q_s,
            q_r,
            (sp, mate),
        )

    q_copy(core).start()
    q2[pl.ds(pl.multiple_of(core * group, group), group), :] = q_held[span]
    top[...] = jnp.full(top.shape, -1e30, F32)
    tot[...] = jnp.zeros(tot.shape, F32)
    acc[...] = jnp.zeros(acc.shape, F32)

    slot_rows = CORES * chips * r

    def attend(slot, slots):
        start = slot * slot_rows
        if not isinstance(start, int):
            start = pl.multiple_of(start, slot_rows)
        here = pl.ds(start, slots * slot_rows)
        scores = lax.dot_general(
            q2[...], kv[here, :head], (((1,), (1,)), ((), ())), preferred_element_type=F32
        ) * (head**-0.5)
        old = top[...]
        new = jnp.maximum(old, jnp.max(scores, axis=-1, keepdims=True))
        shrink = jnp.exp(old - new)
        probs = jnp.exp(scores - new)
        top[...] = new
        tot[...] = tot[...] * shrink + jnp.sum(probs, axis=-1, keepdims=True)
        acc[...] = acc[...] * shrink + jnp.dot(
            probs.astype(BF16), kv[here, head:], preferred_element_type=F32
        )

    def local_loads():
        pairs = [(held, place(core)) for held, place, _ in shared]
        pairs += [(mgain_h, mgain), (fgain_h, fgain)]
        return [load(used + 3 + i, a, b) for i, (a, b) in enumerate(pairs)]

    def mirror_wait(d, start, rows):
        held = kv.at[pl.ds(start, rows), :]
        remote(held, held, d2_s, d2_r.at[d - 1], (sp, mate)).wait_recv()

    def mirrored(d):
        if isinstance(d, int) and d == last:
            begin = (n - 1) * slot_rows

            @pl.when(core == 1)
            def _():
                mirror_wait(d, begin, len(ends) * run)

            if more:

                @pl.when(core == 0)
                def _():
                    mirror_wait(d, begin + len(ends) * run, slot_rows - len(ends) * run)
        else:
            start = slot_of(d, 1 - core) * slot_rows
            mirror_wait(d, pl.multiple_of(start, slot_rows), slot_rows)

    def wave(d):
        for blocks in (own, far):
            for rel in range(CORES):
                arrive(d, rel, blocks)

    if full >= 1:
        feed(4)
        launch_mate(own)
        launch_far()
        feed(3)
        launch_mate(far)
        q_copy(1 - core).wait_recv()
        wave(1)
        rest = local_loads()
        done = 1
        if full > 4:
            wave(2)
            attend(0, 1)

            def middle(d, carry):
                wave(d)
                mirrored(d - 2)
                attend(2 * d - 5, 2)
                return carry

            lax.fori_loop(3, full, middle, 0)
            wave(full)
            done = full - 2
        else:
            for d in range(2, full + 1):
                wave(d)
        start = 2 * done - 1 if full > 4 else 0
        for d in range(done, full):
            mirrored(d)
        attend(start, 2 * full - 1 - start)
        arrive_last()
        feed(len(pending) - SPLIT // 2)
        mirrored(full)
        attend(2 * full - 1, 2)
    else:
        rest = local_loads()
        launch_far()
        launch_mate(range(runs))
        q_copy(1 - core).wait_recv()
        arrive_last()
        feed(3 * SPLIT + 2)
        attend(0, 1)
    if last:
        mirrored(last)
        attend(n - 1, 1)

    attended = (acc[...] / tot[...]).astype(BF16)
    for h in range(CORES * heads_here):
        att[:, h * head : (h + 1) * head] = attended[h * half_rows : (h + 1) * half_rows, :]
    for copy in rest:
        copy.wait()
    shared_wait(0)

    body_rows = half_rows - HALO
    body = slice(0, body_rows)
    tail = slice(body_rows, half_rows)

    def peer_of(k):
        there = chip_at(k)
        return there * CORES + (span + there) % CORES

    def wide_copy(k, c, i):
        at = (body, tail)[i]
        return remote(
            chip_s.at[c, at, :],
            chip_r.at[k - 1, c, at, :],
            bx_s.at[k - 1],
            bx_r.at[k - 1, c * (1 - i) + chunks * i],
            (sp, peer_of(k)),
        )

    for c in range(chunks):
        here = slice(c * cols, (c + 1) * cols)
        product = jnp.dot(att[...], ow[:, here], preferred_element_type=F32)
        chip_s[c] = product.astype(BF16)
        for k in range(1, chips):
            wide_copy(k, c, 1).start()
        res[:, here] = product + tgt[pl.ds(base, half_rows), here].astype(F32)
    for c in range(chunks):
        for k in range(1, chips):
            wide_copy(k, c, 0).start()

    def wide_all(k, at, recv):
        return remote(
            chip_s.at[:, at, :],
            chip_r.at[k - 1, :, at, :],
            bx_s.at[k - 1],
            bx_r.at[k - 1, recv],
            (sp, peer_of(k)),
        )

    def settle(c, i):
        at = (body, tail)[i]
        here = slice(c * cols, (c + 1) * cols)
        residual = res[at, here]
        for k in range(1, chips):
            if i == 0:
                wide_copy(k, c, 0).wait_recv()
            residual = residual + chip_r[k - 1, c, at, :].astype(F32)
        residual = residual.astype(BF16).astype(F32)
        res[at, here] = residual
        return jnp.sum(residual * residual, axis=-1, keepdims=True)

    for k in range(1, chips):
        wide_all(k, tail, chunks).wait_recv()

    beyond = sp * (1 - span) + following * span

    halo = remote(halo_s, rows_in.at[:, 0:HALO, :], h_s, h_r, (beyond, mate))

    sends_halo = jnp.logical_or(span == 0, sp < n - 1)
    takes_halo = jnp.logical_or(span == 1, sp > 0)
    tail_squares = settle(0, 1)
    for c in range(1, chunks):
        tail_squares = tail_squares + settle(c, 1)
    scale = lax.rsqrt(tail_squares / width + EPS)
    for c in range(chunks):
        here = slice(c * cols, (c + 1) * cols)
        halo_s[c] = (res[tail, here] * scale * mgain[:, here]).astype(BF16)

    @pl.when(sends_halo)
    def _():
        halo.start()

    feed(len(pending))

    @pl.when(jnp.logical_not(takes_halo))
    def _():
        rows_in[:, 0:HALO, :] = jnp.zeros((chunks, HALO, cols), BF16)

    def ready():
        @pl.when(takes_halo)
        def _():
            halo.wait_recv()

    def mix(c):
        here = slice(c * cols, (c + 1) * cols)
        for side in range(CORES):
            there = slice(side * ff, (side + 1) * ff)
            for weight, total in ((gw, conv_g), (uw, conv_u)):
                product = jnp.dot(
                    rows_in[c], weight[side, here, :], preferred_element_type=F32
                )
                if c > 0:
                    product = product + total[:, there]
                total[:, there] = product

    for i in range(1, len(shared) - 1):
        shared_wait(i)
    squares = jnp.zeros((body_rows, 1), F32)
    for c in range(chunks):
        squares = squares + settle(c, 0)
        here = slice(c * cols, (c + 1) * cols)
        rows_in[c, HALO:, :] = (res[:, here] * mgain[:, here]).astype(BF16)
        if c == 1:
            ready()
        if 0 < c < chunks - 1:
            for i in range(0 if c == 1 else c, c + 1):
                mix(i)
    squares = jnp.concatenate([squares, tail_squares], axis=0)
    scale = jnp.concatenate(
        [jnp.ones((HALO, 1), F32), lax.rsqrt(squares / width + EPS)], axis=0
    )

    source = tp // chips
    held_row = pl.multiple_of((tp % chips) * rs, rs)
    mate_row = pl.multiple_of((mate % chips) * rs, rs)
    sends_res = mate // chips == span
    holds = source == span

    def res_copy():
        return remote(res_s, res_r, r_s, r_r, (sp, mate))

    @pl.when(sends_res)
    def _():
        res_s[...] = res[pl.ds(mate_row, rs), :].astype(BF16)
        res_copy().start()

    taps = gtaps.shape[1]
    last_rows = slice((chunks - 1) * cols, chunks * cols)
    blocks_here = ff // wide
    for f in range(CORES * blocks_here):
        side = f // blocks_here
        part = slice((f % blocks_here) * wide, (f % blocks_here + 1) * wide)
        here = slice(f * wide, (f + 1) * wide)
        for weight, total in ((gw, conv_g), (uw, conv_u)):
            product = total[:, here] + jnp.dot(
                rows_in[chunks - 1], weight[side, last_rows, part], preferred_element_type=F32
            )
            total[:, here] = (product * scale).astype(BF16).astype(F32)
        gate = jnp.zeros((half_rows, wide), F32)
        up = jnp.zeros((half_rows, wide), F32)
        for t in range(taps):
            begin = HALO - (taps - 1) + t
            rows = slice(begin, begin + half_rows)
            gate = gate + gtaps[side, t : t + 1, part].astype(F32) * conv_g[rows, here]
            up = up + utaps[side, t : t + 1, part].astype(F32) * conv_u[rows, here]
        hid[:, here] = (gate / (1.0 + jnp.exp(-gate)) * up).astype(BF16)

    @pl.when(holds)
    def _():
        end_r[chip] = jnp.zeros(end_r.shape[1:], BF16)

    @pl.when(jnp.logical_not(holds))
    def _():
        kept[...] = jnp.zeros(kept.shape, F32)

    shared_wait(len(shared) - 1)

    def end_copy(i, c, at):
        there = span * chips + i
        return remote(
            end_s.at[c, i * rs : (i + 1) * rs, at],
            end_r.at[chip, c].at[:, at],
            fx_s.at[i],
            fx_r.at[chip, c // (chunks - 1)],
            (sp, there),
        )

    def end_in(k, i):
        at = slice(0, chunks - 1) if i == 0 else slice(chunks - 1, chunks)
        return remote(
            end_s.at[at, 0:rs, :], end_r.at[k, at], fx_s.at[0], fx_r.at[k, i], (sp, mate)
        )

    def end_out(i):
        held = end_s.at[:, i * rs : (i + 1) * rs, :]
        return remote(held, end_r.at[chip], fx_s.at[i], fx_r.at[chip, 0], (sp, mate))

    parts = [(0, 0, cols // 2), (0, cols // 2, cols)]
    parts += [(c, 0, cols) for c in range(1, chunks)]
    for c, low, high in parts:
        at = slice(low, high)
        here = slice(c * cols + low, c * cols + high)
        product = jnp.dot(hid[...], dw[:, here], preferred_element_type=F32)
        end_s[c, :, at] = product.astype(BF16)
        for i in range(chips):

            @pl.when(span * chips + i != tp)
            def _(i=i, c=c, at=at):
                end_copy(i, c, at).start()

            @pl.when(span * chips + i == tp)
            def _(i=i, here=here, product=product):
                kept[:, here] = product[i * rs : (i + 1) * rs, :]

    @pl.when(holds)
    def _():
        kept[...] = kept[...] + res[pl.ds(held_row, rs), :]

    @pl.when(jnp.logical_not(holds))
    def _():
        res_copy().wait_recv()
        kept[...] = res_r[...].astype(F32)

    squares = jnp.zeros((rs, 1), F32)
    sums = []
    for c in range(chunks):
        here = slice(c * cols, (c + 1) * cols)
        if c in (0, chunks - 1):
            for k in range(chips):

                @pl.when(k * CORES + (source + k) % CORES != tp)
                def _(k=k, c=c):
                    end_in(k, c // (chunks - 1)).wait_recv()

        total = kept[:, here]
        for k in range(chips):
            total = total + end_r[k, c].astype(F32)
        squares = squares + jnp.sum(total * total, axis=-1, keepdims=True)
        sums.append(total)
    scale = lax.rsqrt(squares / width + EPS)
    for c in range(chunks):
        here = slice(c * cols, (c + 1) * cols)
        out_ref[:, here] = (sums[c] * scale * fgain[:, here]).astype(BF16)

    def sent(rows, sem):
        held = kv.at[0:rows, :]
        remote(held, held, sem, d2_r.at[0], (sp, mate)).wait_send()

    if chips > 1:
        sent((chips - 1) * r, kx_s)
    q_copy(core).wait_send()
    for i in range(len(shared)):
        pushed(i, core).wait_send()
    for k in range(1, chips):
        wide_all(k, slice(0, half_rows), chunks).wait_send()
    for i in range(chips):

        @pl.when(span * chips + i != tp)
        def _(i=i):
            end_out(i).wait_send()

    @pl.when(sends_halo)
    def _():
        halo.wait_send()

    @pl.when(sends_res)
    def _():
        res_copy().wait_send()

    ring_rows = full * CORES * runs * run
    mirror_rows = ring_rows + runs * run
    for side in range(CORES if last else 1):
        extra = (len(ends) + side * len(more)) * run if last else 0

        @pl.when(jnp.logical_or(core == side, not last))
        def _(extra=extra):
            sent(mirror_rows + extra, d2_s)
            if ring_rows + extra:
                sent(ring_rows + extra, ring_s)


def solution(mesh):
    n = mesh.shape["sp"]
    chips = mesh.shape["tp"] // CORES
    head = 256

    def shards(*args):
        args = [a[None, :] if a.ndim == 1 else a for a in args]
        (target, source, _, _, qw, kw, _, ow, _, gw, _, _, _, dw, _) = args
        tgt_rows, width = target.shape
        r = source.shape[0]
        kv_heads = kw.shape[1] // head
        heads_here = qw.shape[1] // head
        rs = tgt_rows // (CORES * chips)
        half = chips * rs
        cols = width // 4
        chunks = width // cols
        ff = gw.shape[1]
        wide = 256 if ff % 256 == 0 else 128
        q_rows = heads_here * tgt_rows
        sub = max(r // RUN, 1)
        runs = chips * sub
        dma = pltpu.SemaphoreType.DMA
        shapes = [a.shape for a in args]
        for i in (9, 10, 11, 12):
            shapes[i] = (CORES,) + shapes[i]
        for i in (7, 13):
            shapes[i] = (CORES * shapes[i][0], shapes[i][1])
        scratch = [pltpu.VMEM(shape, a.dtype) for shape, a in zip(shapes, args, strict=True)]
        scratch += [
            pltpu.VMEM((kv_heads, r, 2 * head), BF16),
            pltpu.VMEM((n * CORES * chips * r, 2 * head), BF16),
            pltpu.VMEM((q_rows, head), BF16),
            pltpu.VMEM((q_rows, 1), F32),
            pltpu.VMEM((q_rows, 1), F32),
            pltpu.VMEM((q_rows, head), F32),
            pltpu.VMEM((half, CORES * heads_here * head), BF16),
            pltpu.VMEM((chunks, half, cols), BF16),
            pltpu.VMEM((max(chips - 1, 1), chunks, half, cols), BF16),
            pltpu.VMEM((CORES, heads_here * half, head), BF16),
            pltpu.VMEM((half, width), F32),
            pltpu.VMEM((chunks, HALO + half, cols), BF16),
            pltpu.VMEM((chunks, HALO, cols), BF16),
            pltpu.VMEM((HALO + half, CORES * ff), F32),
            pltpu.VMEM((HALO + half, CORES * ff), F32),
            pltpu.VMEM((half, CORES * ff), BF16),
            pltpu.VMEM((chunks, half, cols), BF16),
            pltpu.VMEM((chips, chunks, rs, cols), BF16),
            pltpu.VMEM((rs, width), F32),
            pltpu.VMEM((rs, width), BF16),
            pltpu.VMEM((rs, width), BF16),
            dma((len(args) - 2 + 2 * kv_heads,)),
            dma,
            dma((max(runs - sub, 1), 2)),
            dma,
            dma((max(n // 2, 1), CORES, runs)),
            dma,
            dma((max(n // 2, 1),)),
            dma((runs,)),
        ]
        scratch += [dma] * 2
        scratch += [dma((6,))] * 2
        scratch += [dma((max(chips - 1, 1),)), dma((max(chips - 1, 1), chunks + 1))]
        scratch += [dma] * 4
        scratch += [dma((chips,)), dma((chips, 2))]
        return pl.pallas_call(
            functools.partial(layer, (n, chips, kv_heads, head, heads_here, cols, sub, wide)),
            out_shape=pltpu.VMEM((rs, width), BF16),
            in_specs=[pl.BlockSpec(memory_space=pl.ANY)] * len(args),
            out_specs=pl.BlockSpec(memory_space=pltpu.VMEM),
            scratch_shapes=scratch,
            compiler_params=pltpu.CompilerParams(
                collective_id=0, has_side_effects=True, vmem_limit_bytes=60 * 1024 * 1024
            ),
        )(*args)

    in_specs = (
        P("sp", None),
        P(("sp", "tp"), None),
        P(),
        P(),
        P(None, "tp"),
        P(),
        P(),
        P("tp", None),
        P(),
        P(None, "tp"),
        P(None, "tp"),
        P(None, "tp"),
        P(None, "tp"),
        P("tp", None),
        P(),
    )
    return jax.shard_map(
        shards, mesh=mesh, in_specs=in_specs, out_specs=P(("sp", "tp"), None), check_vma=False
    )
```

```python
import functools

import jax
import jax.numpy as jnp
from jax import lax
from jax.experimental import pallas as pl
from jax.experimental.pallas import tpu as pltpu
from jax.sharding import PartitionSpec as P

MESH = pl.DeviceIdType.MESH
EPS = 1e-06
HALO = 16
RUN = 32
CORES = 2
SPLIT = 8
F32 = jnp.float32
BF16 = jnp.bfloat16


def normed(values, gain):
    wide = values.astype(F32)
    scale = lax.rsqrt(jnp.mean(wide * wide, axis=-1, keepdims=True) + EPS)
    return (wide * scale * gain).astype(BF16)


def layer(
    dims,
    target_h,
    source_h,
    qgain_h,
    sgain_h,
    qw_h,
    kw_h,
    vw_h,
    ow_h,
    mgain_h,
    gw_h,
    uw_h,
    gtaps_h,
    utaps_h,
    dw_h,
    fgain_h,
    out_ref,
    tgt,
    src,
    qgain,
    sgain,
    qw,
    kw,
    vw,
    ow,
    mgain,
    gw,
    uw,
    gtaps,
    utaps,
    dw,
    fgain,
    kvh,
    kv,
    q2,
    top,
    tot,
    acc,
    att,
    chip_s,
    chip_r,
    q_held,
    res,
    rows_in,
    halo_s,
    conv_g,
    conv_u,
    hid,
    end_s,
    end_r,
    kept,
    res_s,
    res_r,
    load_sem,
    kx_s,
    kx_r,
    ring_s,
    ring_r,
    d2_s,
    d2_r,
    d2_first,
    q_s,
    q_r,
    w_s,
    w_r,
    bx_s,
    bx_r,
    h_s,
    h_r,
    r_s,
    r_r,
    fx_s,
    fx_r,
):
    n, chips, kv_heads, head, heads_here, cols, sub, wide = dims
    tgt_rows, width = tgt.shape
    r = src.shape[0]
    rs = tgt_rows // (CORES * chips)
    half_rows = chips * rs
    run = r // sub
    runs = chips * sub
    chunks = width // cols
    ff = gw_h.shape[1]
    sp = lax.axis_index("sp")
    tp = lax.axis_index("tp")
    chip = tp // CORES
    core = tp % CORES
    mate = tp + 1 - 2 * core
    span = (core + chip) % CORES
    base = pl.multiple_of(span * half_rows, half_rows)

    def chip_at(k):
        return (chip + k) % chips

    def ring_at(p):
        if n % 2:
            return p
        upper = p // (n // 2)
        return 2 * (p * (1 - upper) + (n - 1 - p) * upper) + upper

    if n % 2:
        pos = sp
    else:
        pos = (sp // 2) * (1 - sp % 2) + (n - 1 - sp // 2) * (sp % 2)
    ahead = ring_at((pos + 1) % n)
    behind = ring_at((pos + n - 1) % n)

    def load(index, hbm, vmem):
        copy = pltpu.make_async_copy(hbm, vmem, load_sem.at[index])
        copy.start()
        return copy

    def head_of(c):
        return (c * CORES * kv_heads) // (chips * CORES)

    own_head = head_of(chip)
    order = [(own_head + 1 + g) % kv_heads for g in range(kv_heads)]

    def columns(g):
        return pl.ds(pl.multiple_of(g * head, head), head)

    first = [load(0, source_h, src), load(1, sgain_h, sgain)]
    by_head = [
        [
            load(2 + 2 * i, kw_h.at[:, columns(g)], kw.at[:, columns(g)]),
            load(3 + 2 * i, vw_h.at[:, columns(g)], vw.at[:, columns(g)]),
        ]
        for i, g in enumerate(order)
    ]
    used = 2 + 2 * kv_heads

    barrier = pltpu.get_barrier_semaphore()
    following = (sp + 1) % n
    peers = [(ahead, tp), (behind, tp), (sp, mate)]
    peers += [(sp, chip_at(k) * CORES + i) for k in range(1, chips) for i in range(CORES)]
    for peer in peers:
        pl.semaphore_signal(barrier, inc=1, device_id=peer, device_id_type=MESH)

    def remote(source_ref, dest_ref, send, recv, device):
        return pltpu.make_async_remote_copy(
            src_ref=source_ref,
            dst_ref=dest_ref,
            send_sem=send,
            recv_sem=recv,
            device_id=device,
            device_id_type=MESH,
        )

    def block(slot, lineage, j):
        start = ((slot * CORES + lineage) * runs + j) * run
        if not isinstance(start, int):
            start = pl.multiple_of(start, run)
        return kv.at[pl.ds(start, run), :]

    def chip_copy(j, half):
        there = chip_at(j // sub)
        at = slice(half * head, (half + 1) * head)
        return remote(
            kvh.at[head_of(there), (j % sub) * run : (j % sub + 1) * run, at],
            block(0, core, j).at[:, at],
            kx_s,
            kx_r.at[j - sub, half],
            (sp, there * CORES + core),
        )

    last = n // 2 if n % 2 == 0 else 0
    full = (n - 1) // 2
    own = range(sub)
    far = range(sub, runs)
    onward = ahead * (1 - core) + behind * core

    def slot_of(d, side):
        if isinstance(d, int) and d == 0:
            return 0
        if isinstance(d, int) and d == last:
            return n - 1
        return 2 * d - 1 + side

    def ring_copy(d, rel, j):
        lineage = core * (1 - rel) + (1 - core) * rel
        return remote(
            block(slot_of(d - 1, core), lineage, j),
            block(slot_of(d, core), lineage, j),
            ring_s,
            ring_r.at[d - 1, rel, j],
            (onward, tp),
        )

    def mirror_copy(d, rel, j, side):
        lineage = side * (1 - rel) + (1 - side) * rel
        held = block(slot_of(d, side), lineage, j)
        first = isinstance(d, int) and d == 0
        return remote(held, held, d2_s, d2_first.at[j] if first else d2_r.at[d - 1], (sp, mate))

    def mirror_out(d, rel, j):
        return mirror_copy(d, rel, j, core)

    def mirror_in(d, rel, j):
        return mirror_copy(d, rel, j, 1 - core)

    def whole(w, side):
        high = w.shape[0] // CORES
        return w.at[pl.ds(pl.multiple_of(side * high, high), high), :]

    shared = [
        (ow_h, lambda side: whole(ow, side), SPLIT),
        (gw_h, lambda side: gw.at[side], SPLIT),
        (uw_h, lambda side: uw.at[side], SPLIT),
        (gtaps_h, lambda side: gtaps.at[side], 1),
        (utaps_h, lambda side: utaps.at[side], 1),
        (dw_h, lambda side: whole(dw, side), SPLIT),
    ]

    def push(i, p, side):
        held, place, pieces = shared[i]
        high = held.shape[0] // pieces
        at = slice(p * high, (p + 1) * high)
        there = place(side)
        return remote(
            held.at[at, :], there.at[at, :], w_s.at[i], w_r.at[i], (sp, mate)
        )

    def pushed(i, side):
        held, place, _ = shared[i]
        return remote(held, place(side), w_s.at[i], w_r.at[i], (sp, mate))

    pending = [(i, p) for i in range(len(shared)) for p in range(shared[i][2])]

    def feed(count):
        for x in pending[:count]:
            push(*x, core).start()
        del pending[:count]

    def shared_wait(i):
        pushed(i, 1 - core).wait_recv()

    def launch(j):
        if full >= 1 or (last and (0, j) in ends):
            ring_copy(1, 0, j).start()
        elif last:

            @pl.when(core == 1)
            def _():
                ring_copy(1, 0, j).start()

        mirror_out(0, 0, j).start()

    def launch_mate(blocks):
        for j in blocks:
            mirror_in(0, 0, j).wait_recv()
            if full >= 1:
                ring_copy(1, 1, j).start()
            elif last and (1, j) in more:

                @pl.when(core == 1)
                def _(j=j):
                    ring_copy(1, 1, j).start()

    def launch_far():
        for j in far:
            chip_copy(j, 0).wait_recv()
            chip_copy(j, 1).wait_recv()
            launch(j)

    quota = {1: 6, 2: 5, 3: 1}
    ends = [(0, j) for j in own]
    more = [(rel, j) for rel in range(CORES) for j in far]

    def arrive(d, rel, blocks):
        end = isinstance(d, int) and d == full
        for j in blocks:
            ring_copy(d, rel, j).wait_recv()
            if not end or (last and (rel, j) in ends):
                ring_copy(d + 1, rel, j).start()
            elif last and (rel, j) in more:

                @pl.when(core == 1)
                def _(rel=rel, j=j):
                    ring_copy(last, rel, j).start()

            mirror_out(d, rel, j).start()
            if isinstance(d, int) and d in quota and quota[d] > 0:
                quota[d] -= 1
                feed(1)

    def arrive_last():
        if last:
            for rel, j in ends:
                ring_copy(last, rel, j).wait_recv()
                mirror_out(last, rel, j).start()

            if more:

                @pl.when(core == 1)
                def _():
                    for rel, j in more:
                        ring_copy(last, rel, j).wait_recv()
                        mirror_out(last, rel, j).start()

    for copy in first:
        copy.wait()
    source_in = normed(src[...], sgain[...])
    second = [
        load(used + i, a, b)
        for i, (a, b) in enumerate(((target_h, tgt), (qgain_h, qgain), (qw_h, qw)))
    ]
    early = chips == kv_heads

    def send_far(half):
        for j in far:
            chip_copy(j, half).start()

    for i, g in enumerate(order):
        for half, copy in enumerate(by_head[i]):
            if i == 0 or half == 0:
                for waited in by_head[i] if i else [copy]:
                    waited.wait()
            weight = (kw, vw)[half]
            product = jnp.dot(source_in, weight[:, columns(g)], preferred_element_type=F32)
            kvh[g, :, half * head : (half + 1) * head] = product.astype(BF16)
            if i == (kv_heads - 2 if early else kv_heads - 1):
                if half == 0:
                    pl.semaphore_wait(barrier, len(peers))
                send_far(half)
    kv[pl.ds(pl.multiple_of(core * chips * r, r), r), :] = kvh[own_head]
    for j in range(sub):
        launch(j)
    for copy in second:
        copy.wait()
    queries = jnp.dot(normed(tgt[...], qgain[...]), qw[...], preferred_element_type=F32).astype(
        BF16
    )
    group = heads_here * half_rows
    for side in range(CORES):
        for h in range(heads_here):
            q_held[side, h * half_rows : (h + 1) * half_rows, :] = queries[
                side * half_rows : (side + 1) * half_rows, h * head : (h + 1) * head
            ]

    def q_copy(side):
        return remote(
            q_held.at[1 - span],
            q2.at[pl.ds(pl.multiple_of(side * group, group), group), :],
            q_s,
            q_r,
            (sp, mate),
        )

    q_copy(core).start()
    q2[pl.ds(pl.multiple_of(core * group, group), group), :] = q_held[span]
    top[...] = jnp.full(top.shape, -1e30, F32)
    tot[...] = jnp.zeros(tot.shape, F32)
    acc[...] = jnp.zeros(acc.shape, F32)

    slot_rows = CORES * chips * r

    def attend(slot, slots):
        start = slot * slot_rows
        if not isinstance(start, int):
            start = pl.multiple_of(start, slot_rows)
        here = pl.ds(start, slots * slot_rows)
        scores = lax.dot_general(
            q2[...], kv[here, :head], (((1,), (1,)), ((), ())), preferred_element_type=F32
        ) * (head**-0.5)
        old = top[...]
        new = jnp.maximum(old, jnp.max(scores, axis=-1, keepdims=True))
        shrink = jnp.exp(old - new)
        probs = jnp.exp(scores - new)
        top[...] = new
        tot[...] = tot[...] * shrink + jnp.sum(probs, axis=-1, keepdims=True)
        acc[...] = acc[...] * shrink + jnp.dot(
            probs.astype(BF16), kv[here, head:], preferred_element_type=F32
        )

    def local_loads():
        pairs = [(held, place(core)) for held, place, _ in shared]
        pairs += [(mgain_h, mgain), (fgain_h, fgain)]
        return [load(used + 3 + i, a, b) for i, (a, b) in enumerate(pairs)]

    def mirror_wait(d, start, rows):
        held = kv.at[pl.ds(start, rows), :]
        remote(held, held, d2_s, d2_r.at[d - 1], (sp, mate)).wait_recv()

    def mirrored(d):
        if isinstance(d, int) and d == last:
            begin = (n - 1) * slot_rows

            @pl.when(core == 1)
            def _():
                mirror_wait(d, begin, len(ends) * run)

            if more:

                @pl.when(core == 0)
                def _():
                    mirror_wait(d, begin + len(ends) * run, slot_rows - len(ends) * run)
        else:
            start = slot_of(d, 1 - core) * slot_rows
            mirror_wait(d, pl.multiple_of(start, slot_rows), slot_rows)

    def wave(d):
        for blocks in (own, far):
            for rel in range(CORES):
                arrive(d, rel, blocks)

    if full >= 1:
        feed(4)
        launch_mate(own)
        launch_far()
        feed(3)

        @pl.when(core == 0)
        def _():
            launch_mate(far)

        arrive(1, 0, own)

        @pl.when(core == 1)
        def _():
            launch_mate(far)

        q_copy(1 - core).wait_recv()
        arrive(1, 1, own)
        arrive(1, 0, far)
        arrive(1, 1, far)
        rest = local_loads()
        done = 1
        if full > 4:
            wave(2)
            attend(0, 1)

            def middle(d, carry):
                wave(d)
                mirrored(d - 2)
                attend(2 * d - 5, 2)
                return carry

            lax.fori_loop(3, full, middle, 0)
            wave(full)
            done = full - 2
        else:
            for d in range(2, full + 1):
                wave(d)
        start = 2 * done - 1 if full > 4 else 0
        for d in range(done, full):
            mirrored(d)
        attend(start, 2 * full - 1 - start)
        arrive_last()
        feed(len(pending) - SPLIT // 2)
        mirrored(full)
        attend(2 * full - 1, 2)
    else:
        rest = local_loads()
        launch_far()
        launch_mate(range(runs))
        q_copy(1 - core).wait_recv()
        arrive_last()
        feed(3 * SPLIT + 2)
        attend(0, 1)
    if last:
        mirrored(last)
        attend(n - 1, 1)

    attended = (acc[...] / tot[...]).astype(BF16)
    for h in range(CORES * heads_here):
        att[:, h * head : (h + 1) * head] = attended[h * half_rows : (h + 1) * half_rows, :]
    for copy in rest:
        copy.wait()
    shared_wait(0)

    body_rows = half_rows - HALO
    body = slice(0, body_rows)
    tail = slice(body_rows, half_rows)

    def peer_of(k):
        there = chip_at(k)
        return there * CORES + (span + there) % CORES

    def wide_copy(k, c, i):
        at = (body, tail)[i]
        return remote(
            chip_s.at[c, at, :],
            chip_r.at[k - 1, c, at, :],
            bx_s.at[k - 1],
            bx_r.at[k - 1, c * (1 - i) + chunks * i],
            (sp, peer_of(k)),
        )

    for c in range(chunks):
        here = slice(c * cols, (c + 1) * cols)
        product = jnp.dot(att[...], ow[:, here], preferred_element_type=F32)
        chip_s[c] = product.astype(BF16)
        for k in range(1, chips):
            wide_copy(k, c, 1).start()
        res[:, here] = product + tgt[pl.ds(base, half_rows), here].astype(F32)
    for c in range(chunks):
        for k in range(1, chips):
            wide_copy(k, c, 0).start()

    def wide_all(k, at, recv):
        return remote(
            chip_s.at[:, at, :],
            chip_r.at[k - 1, :, at, :],
            bx_s.at[k - 1],
            bx_r.at[k - 1, recv],
            (sp, peer_of(k)),
        )

    def settle(c, i):
        at = (body, tail)[i]
        here = slice(c * cols, (c + 1) * cols)
        residual = res[at, here]
        for k in range(1, chips):
            if i == 0:
                wide_copy(k, c, 0).wait_recv()
            residual = residual + chip_r[k - 1, c, at, :].astype(F32)
        residual = residual.astype(BF16).astype(F32)
        res[at, here] = residual
        return jnp.sum(residual * residual, axis=-1, keepdims=True)

    for k in range(1, chips):
        wide_all(k, tail, chunks).wait_recv()

    beyond = sp * (1 - span) + following * span

    halo = remote(halo_s, rows_in.at[:, 0:HALO, :], h_s, h_r, (beyond, mate))

    sends_halo = jnp.logical_or(span == 0, sp < n - 1)
    takes_halo = jnp.logical_or(span == 1, sp > 0)
    tail_squares = settle(0, 1)
    for c in range(1, chunks):
        tail_squares = tail_squares + settle(c, 1)
    scale = lax.rsqrt(tail_squares / width + EPS)
    for c in range(chunks):
        here = slice(c * cols, (c + 1) * cols)
        halo_s[c] = (res[tail, here] * scale * mgain[:, here]).astype(BF16)

    @pl.when(sends_halo)
    def _():
        halo.start()

    feed(len(pending))

    @pl.when(jnp.logical_not(takes_halo))
    def _():
        rows_in[:, 0:HALO, :] = jnp.zeros((chunks, HALO, cols), BF16)

    def ready():
        @pl.when(takes_halo)
        def _():
            halo.wait_recv()

    def mix(c):
        here = slice(c * cols, (c + 1) * cols)
        for side in range(CORES):
            there = slice(side * ff, (side + 1) * ff)
            for weight, total in ((gw, conv_g), (uw, conv_u)):
                product = jnp.dot(
                    rows_in[c], weight[side, here, :], preferred_element_type=F32
                )
                if c > 0:
                    product = product + total[:, there]
                total[:, there] = product

    for i in range(1, len(shared) - 1):
        shared_wait(i)
    squares = jnp.zeros((body_rows, 1), F32)
    for c in range(chunks):
        squares = squares + settle(c, 0)
        here = slice(c * cols, (c + 1) * cols)
        rows_in[c, HALO:, :] = (res[:, here] * mgain[:, here]).astype(BF16)
        if c == 1:
            ready()
        if 0 < c < chunks - 1:
            for i in range(0 if c == 1 else c, c + 1):
                mix(i)
    squares = jnp.concatenate([squares, tail_squares], axis=0)
    scale = jnp.concatenate(
        [jnp.ones((HALO, 1), F32), lax.rsqrt(squares / width + EPS)], axis=0
    )

    source = tp // chips
    held_row = pl.multiple_of((tp % chips) * rs, rs)
    mate_row = pl.multiple_of((mate % chips) * rs, rs)
    sends_res = mate // chips == span
    holds = source == span

    def res_copy():
        return remote(res_s, res_r, r_s, r_r, (sp, mate))

    @pl.when(sends_res)
    def _():
        res_s[...] = res[pl.ds(mate_row, rs), :].astype(BF16)
        res_copy().start()

    taps = gtaps.shape[1]
    last_rows = slice((chunks - 1) * cols, chunks * cols)
    blocks_here = ff // wide
    for f in range(CORES * blocks_here):
        side = f // blocks_here
        part = slice((f % blocks_here) * wide, (f % blocks_here + 1) * wide)
        here = slice(f * wide, (f + 1) * wide)
        for weight, total in ((gw, conv_g), (uw, conv_u)):
            product = total[:, here] + jnp.dot(
                rows_in[chunks - 1], weight[side, last_rows, part], preferred_element_type=F32
            )
            total[:, here] = (product * scale).astype(BF16).astype(F32)
        gate = jnp.zeros((half_rows, wide), F32)
        up = jnp.zeros((half_rows, wide), F32)
        for t in range(taps):
            begin = HALO - (taps - 1) + t
            rows = slice(begin, begin + half_rows)
            gate = gate + gtaps[side, t : t + 1, part].astype(F32) * conv_g[rows, here]
            up = up + utaps[side, t : t + 1, part].astype(F32) * conv_u[rows, here]
        hid[:, here] = (gate / (1.0 + jnp.exp(-gate)) * up).astype(BF16)

    @pl.when(holds)
    def _():
        end_r[chip] = jnp.zeros(end_r.shape[1:], BF16)

    @pl.when(jnp.logical_not(holds))
    def _():
        kept[...] = jnp.zeros(kept.shape, F32)

    shared_wait(len(shared) - 1)

    def end_copy(i, c, at):
        there = span * chips + i
        return remote(
            end_s.at[c, i * rs : (i + 1) * rs, at],
            end_r.at[chip, c].at[:, at],
            fx_s.at[i],
            fx_r.at[chip, c // (chunks - 1)],
            (sp, there),
        )

    def end_in(k, i):
        at = slice(0, chunks - 1) if i == 0 else slice(chunks - 1, chunks)
        return remote(
            end_s.at[at, 0:rs, :], end_r.at[k, at], fx_s.at[0], fx_r.at[k, i], (sp, mate)
        )

    def end_out(i):
        held = end_s.at[:, i * rs : (i + 1) * rs, :]
        return remote(held, end_r.at[chip], fx_s.at[i], fx_r.at[chip, 0], (sp, mate))

    parts = [(0, 0, cols // 2), (0, cols // 2, cols)]
    parts += [(c, 0, cols) for c in range(1, chunks)]
    for c, low, high in parts:
        at = slice(low, high)
        here = slice(c * cols + low, c * cols + high)
        product = jnp.dot(hid[...], dw[:, here], preferred_element_type=F32)
        end_s[c, :, at] = product.astype(BF16)
        for i in range(chips):

            @pl.when(span * chips + i != tp)
            def _(i=i, c=c, at=at):
                end_copy(i, c, at).start()

            @pl.when(span * chips + i == tp)
            def _(i=i, here=here, product=product):
                kept[:, here] = product[i * rs : (i + 1) * rs, :]

    @pl.when(holds)
    def _():
        kept[...] = kept[...] + res[pl.ds(held_row, rs), :]

    @pl.when(jnp.logical_not(holds))
    def _():
        res_copy().wait_recv()
        kept[...] = res_r[...].astype(F32)

    squares = jnp.zeros((rs, 1), F32)
    sums = []
    for c in range(chunks):
        here = slice(c * cols, (c + 1) * cols)
        if c in (0, chunks - 1):
            for k in range(chips):

                @pl.when(k * CORES + (source + k) % CORES != tp)
                def _(k=k, c=c):
                    end_in(k, c // (chunks - 1)).wait_recv()

        total = kept[:, here]
        for k in range(chips):
            total = total + end_r[k, c].astype(F32)
        squares = squares + jnp.sum(total * total, axis=-1, keepdims=True)
        sums.append(total)
    scale = lax.rsqrt(squares / width + EPS)
    for c in range(chunks):
        here = slice(c * cols, (c + 1) * cols)
        out_ref[:, here] = (sums[c] * scale * fgain[:, here]).astype(BF16)

    def sent(rows, sem):
        held = kv.at[0:rows, :]
        remote(held, held, sem, d2_r.at[0], (sp, mate)).wait_send()

    if chips > 1:
        sent((chips - 1) * r, kx_s)
    q_copy(core).wait_send()
    for i in range(len(shared)):
        pushed(i, core).wait_send()
    for k in range(1, chips):
        wide_all(k, slice(0, half_rows), chunks).wait_send()
    for i in range(chips):

        @pl.when(span * chips + i != tp)
        def _(i=i):
            end_out(i).wait_send()

    @pl.when(sends_halo)
    def _():
        halo.wait_send()

    @pl.when(sends_res)
    def _():
        res_copy().wait_send()

    ring_rows = full * CORES * runs * run
    mirror_rows = ring_rows + runs * run
    for side in range(CORES if last else 1):
        extra = (len(ends) + side * len(more)) * run if last else 0

        @pl.when(jnp.logical_or(core == side, not last))
        def _(extra=extra):
            sent(mirror_rows + extra, d2_s)
            if ring_rows + extra:
                sent(ring_rows + extra, ring_s)


def solution(mesh):
    n = mesh.shape["sp"]
    chips = mesh.shape["tp"] // CORES
    head = 256

    def shards(*args):
        args = [a[None, :] if a.ndim == 1 else a for a in args]
        (target, source, _, _, qw, kw, _, ow, _, gw, _, _, _, dw, _) = args
        tgt_rows, width = target.shape
        r = source.shape[0]
        kv_heads = kw.shape[1] // head
        heads_here = qw.shape[1] // head
        rs = tgt_rows // (CORES * chips)
        half = chips * rs
        cols = width // 4
        chunks = width // cols
        ff = gw.shape[1]
        wide = 256 if ff % 256 == 0 else 128
        q_rows = heads_here * tgt_rows
        sub = max(r // RUN, 1)
        runs = chips * sub
        dma = pltpu.SemaphoreType.DMA
        shapes = [a.shape for a in args]
        for i in (9, 10, 11, 12):
            shapes[i] = (CORES,) + shapes[i]
        for i in (7, 13):
            shapes[i] = (CORES * shapes[i][0], shapes[i][1])
        scratch = [pltpu.VMEM(shape, a.dtype) for shape, a in zip(shapes, args, strict=True)]
        scratch += [
            pltpu.VMEM((kv_heads, r, 2 * head), BF16),
            pltpu.VMEM((n * CORES * chips * r, 2 * head), BF16),
            pltpu.VMEM((q_rows, head), BF16),
            pltpu.VMEM((q_rows, 1), F32),
            pltpu.VMEM((q_rows, 1), F32),
            pltpu.VMEM((q_rows, head), F32),
            pltpu.VMEM((half, CORES * heads_here * head), BF16),
            pltpu.VMEM((chunks, half, cols), BF16),
            pltpu.VMEM((max(chips - 1, 1), chunks, half, cols), BF16),
            pltpu.VMEM((CORES, heads_here * half, head), BF16),
            pltpu.VMEM((half, width), F32),
            pltpu.VMEM((chunks, HALO + half, cols), BF16),
            pltpu.VMEM((chunks, HALO, cols), BF16),
            pltpu.VMEM((HALO + half, CORES * ff), F32),
            pltpu.VMEM((HALO + half, CORES * ff), F32),
            pltpu.VMEM((half, CORES * ff), BF16),
            pltpu.VMEM((chunks, half, cols), BF16),
            pltpu.VMEM((chips, chunks, rs, cols), BF16),
            pltpu.VMEM((rs, width), F32),
            pltpu.VMEM((rs, width), BF16),
            pltpu.VMEM((rs, width), BF16),
            dma((len(args) - 2 + 2 * kv_heads,)),
            dma,
            dma((max(runs - sub, 1), 2)),
            dma,
            dma((max(n // 2, 1), CORES, runs)),
            dma,
            dma((max(n // 2, 1),)),
            dma((runs,)),
        ]
        scratch += [dma] * 2
        scratch += [dma((6,))] * 2
        scratch += [dma((max(chips - 1, 1),)), dma((max(chips - 1, 1), chunks + 1))]
        scratch += [dma] * 4
        scratch += [dma((chips,)), dma((chips, 2))]
        return pl.pallas_call(
            functools.partial(layer, (n, chips, kv_heads, head, heads_here, cols, sub, wide)),
            out_shape=pltpu.VMEM((rs, width), BF16),
            in_specs=[pl.BlockSpec(memory_space=pl.ANY)] * len(args),
            out_specs=pl.BlockSpec(memory_space=pltpu.VMEM),
            scratch_shapes=scratch,
            compiler_params=pltpu.CompilerParams(
                collective_id=0, has_side_effects=True, vmem_limit_bytes=60 * 1024 * 1024
            ),
        )(*args)

    in_specs = (
        P("sp", None),
        P(("sp", "tp"), None),
        P(),
        P(),
        P(None, "tp"),
        P(),
        P(),
        P("tp", None),
        P(),
        P(None, "tp"),
        P(None, "tp"),
        P(None, "tp"),
        P(None, "tp"),
        P("tp", None),
        P(),
    )
    return jax.shard_map(
        shards, mesh=mesh, in_specs=in_specs, out_specs=P(("sp", "tp"), None), check_vma=False
    )
```
